32 devices in a mesh: row: 16 (over z, y, x), col: 2 (over core).
Axes of the slice: x: 2, y: 2, z: 4, core: 2. Of those that a mesh axis runs over, the one named last changes fastest.
Arguments:
- tokens: bfloat16 [2, 6144, 2048], P('col', 'row'), may hold values from -6 to 6
- norm_gain: bfloat16 [2048], replicated, may hold values from 0.099609375 to 1.8984375
- in_weight: bfloat16 [2048, 512], P('row', 'col'), may hold values from -0.125 to 0.125
- out_weight: bfloat16 [512, 2048], P('col', 'row'), may hold values from -0.25 to 0.25
Outputs:
- mixed: bfloat16 [2, 6144, 2048], P('col', 'row')
The draws below stay inside these ranges and needn't reach their ends.
All inputs are finite; a program needn't handle non-finite values.
Results may differ from the reference program's by a relative error of at most 0.013.
Values may be sent and summed in bfloat16 or wider, within the bound.
No kernel may reach another device: no remote copies, remote signals or barrier semaphores. Data moves between devices by JAX's collectives and lax.ppermute only.
A program may use at most 64 MiB of HBM per device.

```python
import jax
import jax.numpy as jnp
from jax import lax

D = 2048
FW = 512
GS = 64
GROUPS = 8
LEN = 6144
BATCH = 2


def block_scale(stream_key, extent, pieces, smallest, largest):
    def one(dim, parts):
        steps = jax.random.uniform(jax.random.fold_in(jax.random.fold_in(stream_key, 6), dim), (parts,), jnp.float32, smallest / len(pieces), largest / len(pieces))
        return jnp.repeat(jnp.exp(steps), extent[dim] // parts).reshape((-1,) + (1,) * (len(extent) - dim - 1))

    level = one(*pieces[0])
    for cut in pieces[1:]:
        level = level * one(*cut)
    return level


def bell_draw(key, extent, spread, limit, cuts=(), dtype=jnp.bfloat16):
    loudness = block_scale(key, extent, cuts, -0.22, 0.18) if cuts else 1.0
    values = jax.random.normal(key, extent, jnp.float32) * spread * loudness
    return jnp.minimum(jnp.maximum(values, -limit), limit).astype(dtype)


def setup_inputs(seed: int = 0) -> dict:
    streams_of = jax.random.split(jax.random.key(seed), 5)
    tokens = bell_draw(streams_of[0], (BATCH, LEN, D), 1.0, 6.0, ((0, 2), (1, 16)))
    norm_gain = jnp.clip(1.0 + 0.18 * jax.random.normal(streams_of[1], (D,), jnp.float32), 0.099609375, 1.8984375).astype(jnp.bfloat16)
    in_weight = bell_draw(streams_of[2], (D, FW), D ** -0.5, 0.125, ((0, 16), (1, 2)))
    out_weight = bell_draw(streams_of[3], (FW, D), FW ** -0.5, 0.25, ((0, 2), (1, 16)))
    return {"tokens": tokens, "norm_gain": norm_gain, "in_weight": in_weight, "out_weight": out_weight}


EPS = 1e-06

def mix_sequence(sequence, norm_gain, in_weight, out_weight):
    widened = sequence.astype(jnp.float32)
    inverse_rms = lax.rsqrt(lax.optimization_barrier(jnp.mean(widened * widened, axis=-1, keepdims=True)) + EPS)
    normed = (widened * inverse_rms * norm_gain.astype(jnp.float32)).astype(jnp.bfloat16)
    projected = jnp.dot(normed, in_weight, preferred_element_type=jnp.float32).astype(jnp.bfloat16)
    grouped = projected.astype(jnp.float32).reshape(LEN, GROUPS, GS)
    spectrum = jnp.fft.fftn(grouped, axes=(0, 2), norm='ortho')
    mixed_real = jnp.real(spectrum).reshape(LEN, FW).astype(jnp.bfloat16)
    return jnp.dot(mixed_real, out_weight, preferred_element_type=jnp.float32).astype(jnp.bfloat16)

def reference(tokens, norm_gain, in_weight, out_weight):
    return lax.map(lambda sequence: mix_sequence(sequence, norm_gain, in_weight, out_weight), tokens)
```

```python
import math

import jax
import jax.numpy as jnp
import numpy as np
from jax import lax
from jax.sharding import PartitionSpec as P

GS = 64
EPS = 1e-06
BF = jnp.bfloat16
F32 = jnp.float32


def angles(left, right, modulus):
    product = np.outer(np.asarray(left, np.int64), np.asarray(right, np.int64)) % modulus
    radians = product.astype(np.float64) * (2.0 * math.pi / modulus)
    return np.cos(radians), np.sin(radians)


def group_tables():
    cos, sin = angles(np.arange(GS), np.arange(GS), GS)
    half = GS // 2
    split = np.concatenate([cos[:, : half + 1], sin[:, 1:half]], axis=1)
    join = np.zeros((GS, GS))
    for j in range(half + 1):
        join[j, j] = 1.0
    for j in range(1, half):
        join[half + j, j] = -1.0
        join[j, GS - j] = 1.0
        join[half + j, GS - j] = 1.0
    return split, join


def spread_half(shard, peers):
    near = peers // 2
    other = lax.ppermute(shard, "row", [(i, i ^ near) for i in range(peers)])
    upper = lax.axis_index("row") >= near
    both = jnp.stack([jnp.where(upper, other, shard), jnp.where(upper, shard, other)])
    copies = jnp.broadcast_to(both[None], (near,) + both.shape)
    groups = [list(range(near)), list(range(near, peers))]
    got = lax.all_to_all(copies, "row", split_axis=0, concat_axis=0, tiled=True, axis_index_groups=groups)
    return got.transpose(1, 0, *range(2, got.ndim)).reshape((peers,) + shard.shape)


def column_parts(own, cols):
    if cols == 2:
        return [own, lax.ppermute(own, "col", [(0, 1), (1, 0)])]
    got = lax.all_gather(own, "col", axis=0, tiled=False)
    return [got[i] for i in range(cols)]


def dot(a, b, dims=((1,), (0,))):
    return lax.dot_general(a, b, (dims, ((), ())), preferred_element_type=F32)


def body(tokens, norm_gain, in_weight, out_weight):
    peers = lax.axis_size("row")
    cols = lax.axis_size("col")
    rows = tokens.shape[1]
    length = rows * peers
    channels = in_weight.shape[1] * cols
    narrow = channels // peers
    inner = rows // peers

    in_own = spread_half(in_weight, peers)
    in_own = in_own.reshape(-1, in_weight.shape[1])
    in_parts = column_parts(in_own, cols)
    out_own = spread_half(out_weight, peers)
    out_own = out_own.transpose(1, 0, 2).reshape(out_weight.shape[0], -1)
    out_parts = column_parts(out_own, cols)

    own_rows = tokens[0].astype(F32)
    inverse_rms = lax.rsqrt(jnp.mean(own_rows * own_rows, axis=-1, keepdims=True) + EPS)
    normed = (own_rows * inverse_rms * norm_gain.astype(F32)).astype(BF)
    projected = jnp.concatenate([dot(normed, part).astype(BF) for part in in_parts], axis=1)

    split, join = group_tables()
    groups = channels // GS
    split_all = jnp.asarray(np.kron(np.eye(groups), split.T), BF)
    join_all = jnp.asarray(np.kron(np.eye(groups), join), BF)
    sums = dot(split_all, projected, ((1,), (1,))).astype(BF)

    got = lax.all_to_all(sums.reshape(peers, narrow, rows), "row", split_axis=0, concat_axis=0, tiled=True)
    small_cos, small_sin = angles(np.arange(peers), np.arange(peers), peers)
    first = jnp.asarray(np.kron(np.concatenate([small_cos, -small_sin]), np.eye(narrow)), BF)
    stage = dot(first, got.reshape(channels, rows)).reshape(2, peers, narrow, rows)
    turn_cos, turn_sin = angles(np.arange(peers), np.arange(rows), length)
    turn_cos = jnp.asarray(turn_cos[:, None, :], F32)
    turn_sin = jnp.asarray(turn_sin[:, None, :], F32)
    real = stage[0] * turn_cos + stage[1] * turn_sin
    imag = stage[1] * turn_cos - stage[0] * turn_sin
    which = (lax.axis_index("row") * narrow + jnp.arange(narrow, dtype=jnp.int32)) % GS
    sine = (which > GS // 2)[None, :, None]
    lead = jnp.where(sine, -imag, real)
    tail = jnp.where(sine, real, imag)
    turned = jnp.concatenate([lead, tail], axis=-1).astype(BF).reshape(channels, 2 * rows)
    long_cos, long_sin = angles(np.arange(rows), np.arange(rows), rows)
    second = jnp.asarray(np.concatenate([long_cos, long_sin], axis=1), BF)
    whole = dot(second, turned, ((1,), (1,))).astype(BF)

    back = lax.all_to_all(whole.reshape(peers, inner, channels), "row", split_axis=0, concat_axis=0, tiled=True)
    back = back.reshape(peers, inner, peers, narrow).transpose(1, 2, 0, 3).reshape(rows, channels)
    mixed_real = (dot(back, join_all) * (1.0 / math.sqrt(length * GS))).astype(BF)
    width = channels // len(out_parts)
    result = sum(
        dot(mixed_real[:, i * width : (i + 1) * width], part) for i, part in enumerate(out_parts)
    )
    return result.astype(BF)[None]


def solution(mesh):
    in_specs = (P("col", "row", None), P(), P("row", "col"), P("col", "row"))
    out_specs = P("col", "row", None)
    return jax.shard_map(body, mesh=mesh, in_specs=in_specs, out_specs=out_specs, check_vma=False)
```

```python
import math

import jax
import jax.numpy as jnp
import numpy as np
from jax import lax
from jax.experimental import pallas as pl
from jax.experimental.pallas import tpu as pltpu
from jax.sharding import PartitionSpec as P

GS = 64
EPS = 1e-06
BF = jnp.bfloat16
F32 = jnp.float32


def angles(left, right, modulus):
    product = np.outer(np.asarray(left, np.int64), np.asarray(right, np.int64)) % modulus
    radians = product.astype(np.float64) * (2.0 * math.pi / modulus)
    return np.cos(radians), np.sin(radians)


def group_tables():
    cos, sin = angles(np.arange(GS), np.arange(GS), GS)
    half = GS // 2
    split = np.concatenate([cos[:, : half + 1], sin[:, 1:half]], axis=1)
    join = np.zeros((GS, GS))
    for j in range(half + 1):
        join[j, j] = 1.0
    for j in range(1, half):
        join[half + j, j] = -1.0
        join[j, GS - j] = 1.0
        join[half + j, GS - j] = 1.0
    return split, join


def spread_half(shard, peers):
    near = peers // 2
    other = lax.ppermute(shard, "row", [(i, i ^ near) for i in range(peers)])
    upper = lax.axis_index("row") >= near
    both = jnp.stack([jnp.where(upper, other, shard), jnp.where(upper, shard, other)])
    copies = jnp.broadcast_to(both[None], (near,) + both.shape)
    groups = [list(range(near)), list(range(near, peers))]
    got = lax.all_to_all(copies, "row", split_axis=0, concat_axis=0, tiled=True, axis_index_groups=groups)
    return got.transpose(1, 0, *range(2, got.ndim)).reshape((peers,) + shard.shape)


def column_parts(own, cols):
    if cols == 2:
        return [own, lax.ppermute(own, "col", [(0, 1), (1, 0)])]
    got = lax.all_gather(own, "col", axis=0, tiled=False)
    return [got[i] for i in range(cols)]


def dot(a, b, dims=((1,), (0,))):
    return lax.dot_general(a, b, (dims, ((), ())), preferred_element_type=F32)


def body_general(tokens, norm_gain, in_weight, out_weight):
    peers = lax.axis_size("row")
    cols = lax.axis_size("col")
    rows = tokens.shape[1]
    length = rows * peers
    channels = in_weight.shape[1] * cols
    narrow = channels // peers
    inner = rows // peers

    in_own = spread_half(in_weight, peers)
    in_own = in_own.reshape(-1, in_weight.shape[1])
    in_parts = column_parts(in_own, cols)
    out_own = spread_half(out_weight, peers)
    out_own = out_own.transpose(1, 0, 2).reshape(out_weight.shape[0], -1)
    out_parts = column_parts(out_own, cols)

    own_rows = tokens[0].astype(F32)
    inverse_rms = lax.rsqrt(jnp.mean(own_rows * own_rows, axis=-1, keepdims=True) + EPS)
    normed = (own_rows * inverse_rms * norm_gain.astype(F32)).astype(BF)
    projected = jnp.concatenate([dot(normed, part).astype(BF) for part in in_parts], axis=1)

    split, join = group_tables()
    groups = channels // GS
    split_all = jnp.asarray(np.kron(np.eye(groups), split.T), BF)
    join_all = jnp.asarray(np.kron(np.eye(groups), join), BF)
    sums = dot(split_all, projected, ((1,), (1,))).astype(BF)

    got = lax.all_to_all(sums.reshape(peers, narrow, rows), "row", split_axis=0, concat_axis=0, tiled=True)
    small_cos, small_sin = angles(np.arange(peers), np.arange(peers), peers)
    first = jnp.asarray(np.kron(np.concatenate([small_cos, -small_sin]), np.eye(narrow)), BF)
    stage = dot(first, got.reshape(channels, rows)).reshape(2, peers, narrow, rows)
    turn_cos, turn_sin = angles(np.arange(peers), np.arange(rows), length)
    turn_cos = jnp.asarray(turn_cos[:, None, :], F32)
    turn_sin = jnp.asarray(turn_sin[:, None, :], F32)
    real = stage[0] * turn_cos + stage[1] * turn_sin
    imag = stage[1] * turn_cos - stage[0] * turn_sin
    which = (lax.axis_index("row") * narrow + jnp.arange(narrow, dtype=jnp.int32)) % GS
    sine = (which > GS // 2)[None, :, None]
    lead = jnp.where(sine, -imag, real)
    tail = jnp.where(sine, real, imag)
    turned = jnp.concatenate([lead, tail], axis=-1).astype(BF).reshape(channels, 2 * rows)
    long_cos, long_sin = angles(np.arange(rows), np.arange(rows), rows)
    second = jnp.asarray(np.concatenate([long_cos, long_sin], axis=1), BF)
    whole = dot(second, turned, ((1,), (1,))).astype(BF)

    back = lax.all_to_all(whole.reshape(peers, inner, channels), "row", split_axis=0, concat_axis=0, tiled=True)
    back = back.reshape(peers, inner, peers, narrow).transpose(1, 2, 0, 3).reshape(rows, channels)
    mixed_real = (dot(back, join_all) * (1.0 / math.sqrt(length * GS))).astype(BF)
    width = channels // len(out_parts)
    result = sum(
        dot(mixed_real[:, i * width : (i + 1) * width], part) for i, part in enumerate(out_parts)
    )
    return result.astype(BF)[None]


def swap(value, axis, count, bit):
    return lax.ppermute(value, axis, [(i, i ^ bit) for i in range(count)])


def vmem_params():
    return pltpu.CompilerParams(vmem_limit_bytes=24 * 2**20)


def whole_specs(count):
    return [pl.BlockSpec(memory_space=pltpu.VMEM)] * count


def cost(flops, moved):
    return pl.CostEstimate(flops=int(flops), bytes_accessed=int(moved), transcendentals=0)


def norm_kernel(tokens_ref, gain_ref, out_ref):
    rows = tokens_ref[0].astype(F32)
    inverse_rms = lax.rsqrt(jnp.mean(rows * rows, axis=-1, keepdims=True) + EPS)
    out_ref[...] = (rows * inverse_rms * gain_ref[...].astype(F32)).astype(BF)


def norm_rows(tokens, gain):
    rows, width = tokens.shape[1:]
    step = rows // 6
    return pl.pallas_call(
        norm_kernel,
        out_shape=jax.ShapeDtypeStruct((rows, width), BF),
        grid=(rows // step,),
        in_specs=[
            pl.BlockSpec((1, step, width), lambda i: (0, i, 0)),
            pl.BlockSpec((1, width), lambda i: (0, 0)),
        ],
        out_specs=pl.BlockSpec((step, width), lambda i: (i, 0)),
        compiler_params=vmem_params(),
        cost_estimate=cost(rows * width * 2000, rows * width * 4),
        name="norm_rows",
    )(tokens, gain.reshape(1, width))


def project(me, normed, weight, split, half, into=None):
    near, depth, columns = weight.shape
    depth //= 2
    rows = normed.shape[0]

    def kernel(me_ref, normed_ref, weight_ref, split_ref, *rest):
        out_ref = rest[-1]
        upper = me_ref[0] // near
        total = jnp.zeros((rows, columns), F32)
        for s in range(near):
            own = pl.multiple_of((upper * near + s) * depth, depth)
            far = pl.multiple_of(((1 - upper) * near + s) * depth, depth)
            piece = jnp.concatenate([normed_ref[:, pl.ds(own, depth)], normed_ref[:, pl.ds(far, depth)]], axis=1)
            total = total + jnp.dot(piece, weight_ref[s], preferred_element_type=F32)
        sums = dot(split_ref[...], total.astype(BF), ((1,), (1,)))
        out_ref[...] = sums.astype(BF)

    args = [me, normed, weight, split] + ([] if into is None else [into])
    smem = pl.BlockSpec(memory_space=pltpu.SMEM)
    extra = [] if into is None else [pl.BlockSpec(memory_space=pl.ANY)]
    zero = lambda i: (0, 0)
    return pl.pallas_call(
        kernel,
        out_shape=jax.ShapeDtypeStruct((2 * columns, rows), BF),
        grid=(1,),
        in_specs=[
            smem,
            pl.BlockSpec(normed.shape, zero),
            pl.BlockSpec(weight.shape, lambda i: (0, 0, 0)),
            pl.BlockSpec(split.shape, zero),
        ]
        + extra,
        out_specs=pl.BlockSpec((columns, rows), lambda i: (half, 0)),
        input_output_aliases={} if into is None else {4: 0},
        compiler_params=vmem_params(),
        cost_estimate=cost(2 * rows * near * 2 * depth * columns, weight.size * 2),
        name="project",
    )(*args)


def transform_kernel(narrow, me_ref, got_ref, first_ref, cos_ref, sin_ref, second_ref, out_ref):
    peers, _, rows = cos_ref.shape
    stage = jnp.dot(first_ref[...], got_ref[...], preferred_element_type=F32)
    stage = stage.reshape(2, peers, narrow, rows)
    cos, sin = cos_ref[...], sin_ref[...]
    real = stage[0] * cos + stage[1] * sin
    imag = stage[1] * cos - stage[0] * sin
    which = lax.broadcasted_iota(jnp.int32, (1, narrow, rows), 1) + me_ref[0] * narrow
    sine = lax.rem(which, GS) > GS // 2
    lead = jnp.where(sine, -imag, real).reshape(peers * narrow, rows).astype(BF)
    tail = jnp.where(sine, real, imag).reshape(peers * narrow, rows).astype(BF)
    lanes = ((1,), (1,))
    out = dot(second_ref[:, :rows], lead, lanes) + dot(second_ref[:, rows:], tail, lanes)
    out_ref[...] = out.astype(BF)


def transform(me, got, peers, rows):
    channels = got.shape[0]
    narrow = channels // peers
    small_cos, small_sin = angles(np.arange(peers), np.arange(peers), peers)
    first = jnp.asarray(np.kron(np.concatenate([small_cos, -small_sin]), np.eye(narrow)), BF)
    turn_cos, turn_sin = angles(np.arange(peers), np.arange(rows), rows * peers)
    long_cos, long_sin = angles(np.arange(rows), np.arange(rows), rows)
    second = jnp.asarray(np.concatenate([long_cos, long_sin], axis=1), BF)
    turns = [jnp.asarray(t[:, None, :], F32) for t in (turn_cos, turn_sin)]

    def kernel(*refs):
        transform_kernel(narrow, *refs)

    return pl.pallas_call(
        kernel,
        out_shape=jax.ShapeDtypeStruct((rows, channels), BF),
        in_specs=[pl.BlockSpec(memory_space=pltpu.SMEM)] + whole_specs(5),
        out_specs=pl.BlockSpec(memory_space=pltpu.VMEM),
        compiler_params=vmem_params(),
        cost_estimate=cost(4 * rows * channels * channels, 6 * channels * channels),
        name="transform",
    )(me, got, first, *turns, second)


def regroup(quads, lane):
    low, high = [], []
    for j in range(2):
        a, b = quads[j], quads[j + 2]
        low.append(jnp.where(lane < 64, a, pltpu.roll(b, 64, 1)))
        high.append(jnp.where(lane < 64, pltpu.roll(a, 64, 1), b))
    out = []
    even = lax.rem(lane, 64) < 32
    for e, o in (low, high):
        out.append(jnp.where(even, e, pltpu.roll(o, 32, 1)))
        out.append(jnp.where(even, pltpu.roll(e, 96, 1), o))
    return out


def output_kernel(scale, depth, me_ref, back_ref, join_ref, *refs):
    own, other, (out_ref, sheet) = refs[:8], refs[8:16], refs[16:]
    peers, inner, channels = back_ref.shape
    lane = lax.broadcasted_iota(jnp.int32, (inner, 128), 1)
    quads = channels // 128
    for a in range(quads):
        made = []
        for b in range(quads):
            tiles = [back_ref[4 * b + j, :, 128 * a : 128 * a + 128].astype(F32) for j in range(4)]
            made.append(regroup(tiles, lane))
        for i in range(4):
            for b in range(quads):
                sheet[b, pl.ds(4 * a + i, inner, stride=peers), :] = made[b][i]
    lines = jnp.concatenate([sheet[b].astype(BF) for b in range(quads)], axis=1)
    mixed_real = jnp.dot(lines, join_ref[...], preferred_element_type=F32) * scale
    mixed_real = mixed_real.astype(BF)
    near = len(own)
    upper = me_ref[0] // near
    place = lax.rem(me_ref[0], near)
    width = own[0].shape[2]
    for m in range(near):
        left = jnp.concatenate([own[m][0], own[m][1]], axis=1)
        right = jnp.concatenate([other[m][0], other[m][1]], axis=1)
        part = jnp.dot(mixed_real[:, :depth], left, preferred_element_type=F32)
        part = part + jnp.dot(mixed_real[:, depth:], right, preferred_element_type=F32)
        part = part.astype(BF)
        at = lax.bitwise_xor(place, m)
        here = pl.multiple_of((upper * near + at) * width, width)
        there = pl.multiple_of(((1 - upper) * near + at) * width, width)
        out_ref[:, pl.ds(here, width)] = part[:, :width]
        out_ref[:, pl.ds(there, width)] = part[:, width:]


def output(me, back, join, own, other, scale):
    peers, inner, channels = back.shape
    depth, width = own[0].shape[1:]
    rows = peers * inner

    def kernel(*refs):
        output_kernel(scale, depth, *refs)

    return pl.pallas_call(
        kernel,
        out_shape=jax.ShapeDtypeStruct((rows, width * peers), BF),
        in_specs=[pl.BlockSpec(memory_space=pltpu.SMEM)] + whole_specs(2 + len(own) + len(other)),
        out_specs=pl.BlockSpec(memory_space=pltpu.VMEM),
        scratch_shapes=[pltpu.VMEM((channels // 128, rows, 128), F32)],
        compiler_params=vmem_params(),
        cost_estimate=cost(2 * rows * channels * width * peers, rows * width * peers * 2),
        name="output",
    )(me, back, join, *own, *other)


def body_cube(tokens, norm_gain, in_weight, out_weight):
    peers = lax.axis_size("row")
    cols = lax.axis_size("col")
    near = peers // 2
    rows = tokens.shape[1]
    channels = in_weight.shape[1] * cols
    narrow = channels // peers
    inner = rows // peers
    me = lax.axis_index("row").astype(jnp.int32).reshape(1)
    split, join = group_tables()
    split_half = jnp.asarray(np.kron(np.eye(channels // cols // GS), split.T), BF)
    join_all = jnp.asarray(np.kron(np.eye(channels // GS), join), BF)

    def row_swap(value, bit):
        return swap(value, "row", peers, bit)

    def core_swap(value):
        return swap(value, "col", cols, 1)

    in_both = jnp.stack([in_weight, row_swap(in_weight, near)])
    in_both = in_both.reshape(1, 2 * in_weight.shape[0], in_weight.shape[1])
    groups = [list(range(near)), list(range(near, peers))]
    in_own = lax.all_to_all(
        jnp.broadcast_to(in_both, (near,) + in_both.shape[1:]),
        "row",
        split_axis=0,
        concat_axis=0,
        tiled=True,
        axis_index_groups=groups,
    )
    normed = norm_rows(tokens, norm_gain)
    in_other = core_swap(in_own)

    pairs = {0: jnp.stack([out_weight, row_swap(out_weight, near)])}
    for bit in (1, 2, 4):
        pairs[bit] = row_swap(pairs[0], bit)
    pairs[3] = row_swap(pairs[2], 1)
    pairs[6] = row_swap(pairs[4], 2)
    pairs[5] = row_swap(pairs[1], 4)
    pairs[7] = row_swap(pairs[6], 1)
    others = [core_swap(pairs[m]) for m in range(near)]

    sums = project(me, normed, in_own, split_half, 0)
    sums = project(me, normed, in_other, split_half, 1, sums)
    got = lax.all_to_all(sums.reshape(peers, narrow, rows), "row", split_axis=0, concat_axis=0, tiled=True)
    whole = transform(me, got.reshape(channels, rows), peers, rows)
    back = lax.all_to_all(whole.reshape(peers, inner, channels), "row", split_axis=0, concat_axis=0, tiled=True)
    scale = 1.0 / math.sqrt(rows * peers * GS)
    result = output(me, back, join_all, [pairs[m] for m in range(near)], others, scale)
    return result[None]


def body(tokens, norm_gain, in_weight, out_weight):
    peers, cols = lax.axis_size("row"), lax.axis_size("col")
    channels = in_weight.shape[1] * cols
    fits = tokens.shape[1] % (8 * peers) == 0 and in_weight.shape[0] % 128 == 0 and out_weight.shape[1] % 128 == 0
    if peers == 16 and cols == 2 and channels == 32 * peers and fits:
        return body_cube(tokens, norm_gain, in_weight, out_weight)
    return body_general(tokens, norm_gain, in_weight, out_weight)


def solution(mesh):
    in_specs = (P("col", "row", None), P(), P("row", "col"), P("col", "row"))
    out_specs = P("col", "row", None)
    return jax.shard_map(body, mesh=mesh, in_specs=in_specs, out_specs=out_specs, check_vma=False)
```

```python
import math

import jax
import jax.numpy as jnp
import numpy as np
from jax import lax
from jax.experimental import pallas as pl
from jax.experimental.pallas import tpu as pltpu
from jax.sharding import PartitionSpec as P


GS = 64
EPS = 1e-06
BF = jnp.bfloat16
F32 = jnp.float32


def angles(left, right, modulus):
    product = np.outer(np.asarray(left, np.int64), np.asarray(right, np.int64)) % modulus
    radians = product.astype(np.float64) * (2.0 * math.pi / modulus)
    return np.cos(radians), np.sin(radians)


def group_tables():
    cos, sin = angles(np.arange(GS), np.arange(GS), GS)
    half = GS // 2
    split = np.concatenate([cos[:, : half + 1], sin[:, 1:half]], axis=1)
    join = np.zeros((GS, GS))
    for j in range(half + 1):
        join[j, j] = 1.0
    for j in range(1, half):
        join[half + j, j] = -1.0
        join[j, GS - j] = 1.0
        join[half + j, GS - j] = 1.0
    return split, join


def spread_half(shard, peers):
    near = peers // 2
    other = lax.ppermute(shard, "row", [(i, i ^ near) for i in range(peers)])
    upper = lax.axis_index("row") >= near
    both = jnp.stack([jnp.where(upper, other, shard), jnp.where(upper, shard, other)])
    copies = jnp.broadcast_to(both[None], (near,) + both.shape)
    groups = [list(range(near)), list(range(near, peers))]
    got = lax.all_to_all(copies, "row", split_axis=0, concat_axis=0, tiled=True, axis_index_groups=groups)
    return got.transpose(1, 0, *range(2, got.ndim)).reshape((peers,) + shard.shape)


def column_parts(own, cols):
    if cols == 2:
        return [own, lax.ppermute(own, "col", [(0, 1), (1, 0)])]
    got = lax.all_gather(own, "col", axis=0, tiled=False)
    return [got[i] for i in range(cols)]


def dot(a, b, dims=((1,), (0,))):
    return lax.dot_general(a, b, (dims, ((), ())), preferred_element_type=F32)


def body_general(tokens, norm_gain, in_weight, out_weight):
    peers = lax.axis_size("row")
    cols = lax.axis_size("col")
    rows = tokens.shape[1]
    length = rows * peers
    channels = in_weight.shape[1] * cols
    narrow = channels // peers
    inner = rows // peers

    in_own = spread_half(in_weight, peers)
    in_own = in_own.reshape(-1, in_weight.shape[1])
    in_parts = column_parts(in_own, cols)
    out_own = spread_half(out_weight, peers)
    out_own = out_own.transpose(1, 0, 2).reshape(out_weight.shape[0], -1)
    out_parts = column_parts(out_own, cols)

    own_rows = tokens[0].astype(F32)
    inverse_rms = lax.rsqrt(jnp.mean(own_rows * own_rows, axis=-1, keepdims=True) + EPS)
    normed = (own_rows * inverse_rms * norm_gain.astype(F32)).astype(BF)
    projected = jnp.concatenate([dot(normed, part).astype(BF) for part in in_parts], axis=1)

    split, join = group_tables()
    groups = channels // GS
    split_all = jnp.asarray(np.kron(np.eye(groups), split.T), BF)
    join_all = jnp.asarray(np.kron(np.eye(groups), join), BF)
    sums = dot(split_all, projected, ((1,), (1,))).astype(BF)

    got = lax.all_to_all(sums.reshape(peers, narrow, rows), "row", split_axis=0, concat_axis=0, tiled=True)
    small_cos, small_sin = angles(np.arange(peers), np.arange(peers), peers)
    first = jnp.asarray(np.kron(np.concatenate([small_cos, -small_sin]), np.eye(narrow)), BF)
    stage = dot(first, got.reshape(channels, rows)).reshape(2, peers, narrow, rows)
    turn_cos, turn_sin = angles(np.arange(peers), np.arange(rows), length)
    turn_cos = jnp.asarray(turn_cos[:, None, :], F32)
    turn_sin = jnp.asarray(turn_sin[:, None, :], F32)
    real = stage[0] * turn_cos + stage[1] * turn_sin
    imag = stage[1] * turn_cos - stage[0] * turn_sin
    which = (lax.axis_index("row") * narrow + jnp.arange(narrow, dtype=jnp.int32)) % GS
    sine = (which > GS // 2)[None, :, None]
    lead = jnp.where(sine, -imag, real)
    tail = jnp.where(sine, real, imag)
    turned = jnp.concatenate([lead, tail], axis=-1).astype(BF).reshape(channels, 2 * rows)
    long_cos, long_sin = angles(np.arange(rows), np.arange(rows), rows)
    second = jnp.asarray(np.concatenate([long_cos, long_sin], axis=1), BF)
    whole = dot(second, turned, ((1,), (1,))).astype(BF)

    back = lax.all_to_all(whole.reshape(peers, inner, channels), "row", split_axis=0, concat_axis=0, tiled=True)
    back = back.reshape(peers, inner, peers, narrow).transpose(1, 2, 0, 3).reshape(rows, channels)
    mixed_real = (dot(back, join_all) * (1.0 / math.sqrt(length * GS))).astype(BF)
    width = channels // len(out_parts)
    result = sum(
        dot(mixed_real[:, i * width : (i + 1) * width], part) for i, part in enumerate(out_parts)
    )
    return result.astype(BF)[None]


def swap(value, axis, count, bit):
    return lax.ppermute(value, axis, [(i, i ^ bit) for i in range(count)])


def vmem_params():
    return pltpu.CompilerParams(vmem_limit_bytes=24 * 2**20)


def whole_specs(count):
    return [pl.BlockSpec(memory_space=pltpu.VMEM)] * count


def cost(flops, moved):
    return pl.CostEstimate(flops=int(flops), bytes_accessed=int(moved), transcendentals=0)


def norm_kernel(tokens_ref, gain_ref, out_ref):
    rows = tokens_ref[0].astype(F32)
    inverse_rms = lax.rsqrt(jnp.mean(rows * rows, axis=-1, keepdims=True) + EPS)
    out_ref[...] = (rows * inverse_rms * gain_ref[...].astype(F32)).astype(BF)


def norm_rows(tokens, gain):
    rows, width = tokens.shape[1:]
    step = rows // 6
    return pl.pallas_call(
        norm_kernel,
        out_shape=jax.ShapeDtypeStruct((rows, width), BF),
        grid=(rows // step,),
        in_specs=[
            pl.BlockSpec((1, step, width), lambda i: (0, i, 0)),
            pl.BlockSpec((1, width), lambda i: (0, 0)),
        ],
        out_specs=pl.BlockSpec((step, width), lambda i: (i, 0)),
        compiler_params=vmem_params(),
        cost_estimate=cost(rows * width * 2000, rows * width * 4),
        name="norm_rows",
    )(tokens, gain.reshape(1, width))


def project(me, normed, weight, split, half, into=None):
    near, depth, columns = weight.shape
    depth //= 2
    rows = normed.shape[0]

    def kernel(me_ref, normed_ref, weight_ref, split_ref, *rest):
        out_ref = rest[-1]
        upper = me_ref[0] // near
        total = jnp.zeros((rows, columns), F32)
        for s in range(near):
            own = pl.multiple_of((upper * near + s) * depth, depth)
            far = pl.multiple_of(((1 - upper) * near + s) * depth, depth)
            piece = jnp.concatenate([normed_ref[:, pl.ds(own, depth)], normed_ref[:, pl.ds(far, depth)]], axis=1)
            total = total + jnp.dot(piece, weight_ref[s], preferred_element_type=F32)
        sums = dot(split_ref[...], total.astype(BF), ((1,), (1,)))
        out_ref[...] = sums.astype(BF)

    args = [me, normed, weight, split] + ([] if into is None else [into])
    smem = pl.BlockSpec(memory_space=pltpu.SMEM)
    extra = [] if into is None else [pl.BlockSpec(memory_space=pl.ANY)]
    zero = lambda i: (0, 0)
    return pl.pallas_call(
        kernel,
        out_shape=jax.ShapeDtypeStruct((2 * columns, rows), BF),
        grid=(1,),
        in_specs=[
            smem,
            pl.BlockSpec(normed.shape, zero),
            pl.BlockSpec(weight.shape, lambda i: (0, 0, 0)),
            pl.BlockSpec(split.shape, zero),
        ]
        + extra,
        out_specs=pl.BlockSpec((columns, rows), lambda i: (half, 0)),
        input_output_aliases={} if into is None else {4: 0},
        compiler_params=vmem_params(),
        cost_estimate=cost(2 * rows * near * 2 * depth * columns, weight.size * 2),
        name="project",
    )(*args)


def transform_kernel(narrow, me_ref, got_ref, first_ref, cos_ref, sin_ref, second_ref, out_ref):
    peers, _, rows = cos_ref.shape
    stage = jnp.dot(first_ref[...], got_ref[...], preferred_element_type=F32)
    stage = stage.reshape(2, peers, narrow, rows)
    cos, sin = cos_ref[...], sin_ref[...]
    real = stage[0] * cos + stage[1] * sin
    imag = stage[1] * cos - stage[0] * sin
    which = lax.broadcasted_iota(jnp.int32, (1, narrow, rows), 1) + me_ref[0] * narrow
    sine = lax.rem(which, GS) > GS // 2
    lead = jnp.where(sine, -imag, real).reshape(peers * narrow, rows).astype(BF)
    tail = jnp.where(sine, real, imag).reshape(peers * narrow, rows).astype(BF)
    lanes = ((1,), (1,))
    out = dot(second_ref[:, :rows], lead, lanes) + dot(second_ref[:, rows:], tail, lanes)
    out_ref[...] = out.astype(BF)


def transform(me, got, peers, rows):
    channels = got.shape[0]
    narrow = channels // peers
    small_cos, small_sin = angles(np.arange(peers), np.arange(peers), peers)
    first = jnp.asarray(np.kron(np.concatenate([small_cos, -small_sin]), np.eye(narrow)), BF)
    turn_cos, turn_sin = angles(np.arange(peers), np.arange(rows), rows * peers)
    long_cos, long_sin = angles(np.arange(rows), np.arange(rows), rows)
    second = jnp.asarray(np.concatenate([long_cos, long_sin], axis=1), BF)
    turns = [jnp.asarray(t[:, None, :], F32) for t in (turn_cos, turn_sin)]

    def kernel(*refs):
        transform_kernel(narrow, *refs)

    return pl.pallas_call(
        kernel,
        out_shape=jax.ShapeDtypeStruct((rows, channels), BF),
        in_specs=[pl.BlockSpec(memory_space=pltpu.SMEM)] + whole_specs(5),
        out_specs=pl.BlockSpec(memory_space=pltpu.VMEM),
        compiler_params=vmem_params(),
        cost_estimate=cost(4 * rows * channels * channels, 6 * channels * channels),
        name="transform",
    )(me, got, first, *turns, second)


def regroup(quads, lane):
    low, high = [], []
    for j in range(2):
        a, b = quads[j], quads[j + 2]
        low.append(jnp.where(lane < 64, a, pltpu.roll(b, 64, 1)))
        high.append(jnp.where(lane < 64, pltpu.roll(a, 64, 1), b))
    out = []
    even = lax.rem(lane, 64) < 32
    for e, o in (low, high):
        out.append(jnp.where(even, e, pltpu.roll(o, 32, 1)))
        out.append(jnp.where(even, pltpu.roll(e, 96, 1), o))
    return out


def output_kernel(scale, depth, me_ref, back_ref, join_ref, *refs):
    own, (other_a, other_b, other_c), (out_ref, sheet) = refs[:8], refs[8:11], refs[11:]
    other = {7: other_c}
    for i, m in enumerate((0, 1, 2, 4)):
        other[m] = other_a.at[2 * i : 2 * i + 2]
    for i, m in enumerate((3, 5, 6)):
        other[m] = other_b.at[2 * i : 2 * i + 2]
    peers, inner, channels = back_ref.shape
    lane = lax.broadcasted_iota(jnp.int32, (inner, 128), 1)
    quads = channels // 128
    for a in range(quads):
        made = []
        for b in range(quads):
            tiles = [back_ref[4 * b + j, :, 128 * a : 128 * a + 128].astype(F32) for j in range(4)]
            made.append(regroup(tiles, lane))
        for i in range(4):
            for b in range(quads):
                sheet[b, pl.ds(4 * a + i, inner, stride=peers), :] = made[b][i]
    lines = jnp.concatenate([sheet[b].astype(BF) for b in range(quads)], axis=1)
    mixed_real = jnp.dot(lines, join_ref[...], preferred_element_type=F32) * scale
    mixed_real = mixed_real.astype(BF)
    near = len(own)
    upper = me_ref[0] // near
    place = lax.rem(me_ref[0], near)
    width = own[0].shape[2]
    for m in range(near):
        left = jnp.concatenate([own[m][0], own[m][1]], axis=1)
        right = jnp.concatenate([other[m][0], other[m][1]], axis=1)
        part = jnp.dot(mixed_real[:, :depth], left, preferred_element_type=F32)
        part = part + jnp.dot(mixed_real[:, depth:], right, preferred_element_type=F32)
        part = part.astype(BF)
        at = lax.bitwise_xor(place, m)
        here = pl.multiple_of((upper * near + at) * width, width)
        there = pl.multiple_of(((1 - upper) * near + at) * width, width)
        out_ref[:, pl.ds(here, width)] = part[:, :width]
        out_ref[:, pl.ds(there, width)] = part[:, width:]


def output(me, back, join, own, other, scale):
    peers, inner, channels = back.shape
    depth, width = own[0].shape[1:]
    rows = peers * inner

    def kernel(*refs):
        output_kernel(scale, depth, *refs)

    return pl.pallas_call(
        kernel,
        out_shape=jax.ShapeDtypeStruct((rows, width * peers), BF),
        in_specs=[pl.BlockSpec(memory_space=pltpu.SMEM)] + whole_specs(2 + len(own) + len(other)),
        out_specs=pl.BlockSpec(memory_space=pltpu.VMEM),
        scratch_shapes=[pltpu.VMEM((channels // 128, rows, 128), F32)],
        compiler_params=vmem_params(),
        cost_estimate=cost(2 * rows * channels * width * peers, rows * width * peers * 2),
        name="output",
    )(me, back, join, *own, *other)


def body_cube(tokens, norm_gain, in_weight, out_weight):
    peers = lax.axis_size("row")
    cols = lax.axis_size("col")
    near = peers // 2
    rows = tokens.shape[1]
    channels = in_weight.shape[1] * cols
    narrow = channels // peers
    inner = rows // peers
    me = lax.axis_index("row").astype(jnp.int32).reshape(1)
    split, join = group_tables()
    split_half = jnp.asarray(np.kron(np.eye(channels // cols // GS), split.T), BF)
    join_all = jnp.asarray(np.kron(np.eye(channels // GS), join), BF)

    def row_swap(value, bit):
        return swap(value, "row", peers, bit)

    def core_swap(value):
        return swap(value, "col", cols, 1)

    in_both = jnp.stack([in_weight, row_swap(in_weight, near)])
    in_both = in_both.reshape(1, 2 * in_weight.shape[0], in_weight.shape[1])
    groups = [list(range(near)), list(range(near, peers))]
    in_own = lax.all_to_all(
        jnp.broadcast_to(in_both, (near,) + in_both.shape[1:]),
        "row",
        split_axis=0,
        concat_axis=0,
        tiled=True,
        axis_index_groups=groups,
    )
    normed = norm_rows(tokens, norm_gain)
    in_other = core_swap(in_own)

    out_far = row_swap(out_weight, near)
    pairs = {0: jnp.stack([out_weight, out_far])}
    for bit in (1, 2, 4):
        pairs[bit] = row_swap(pairs[0], bit)
    pairs[3] = row_swap(pairs[2], 1)
    pairs[6] = row_swap(pairs[4], 2)
    pairs[5] = row_swap(pairs[1], 4)
    pairs[7] = row_swap(pairs[6], 1)
    first = jnp.concatenate([pairs[m] for m in (0, 1, 2, 4)])
    second = jnp.concatenate([pairs[m] for m in (3, 5, 6)])
    others = [core_swap(value) for value in (first, second, pairs[7])]

    sums = project(me, normed, in_own, split_half, 0)
    sums = project(me, normed, in_other, split_half, 1, sums)
    got = lax.all_to_all(sums.reshape(peers, narrow, rows), "row", split_axis=0, concat_axis=0, tiled=True)
    whole = transform(me, got.reshape(channels, rows), peers, rows)
    back = lax.all_to_all(whole.reshape(peers, inner, channels), "row", split_axis=0, concat_axis=0, tiled=True)
    scale = 1.0 / math.sqrt(rows * peers * GS)
    result = output(me, back, join_all, [pairs[m] for m in range(near)], others, scale)
    return result[None]


def body(tokens, norm_gain, in_weight, out_weight):
    peers, cols = lax.axis_size("row"), lax.axis_size("col")
    channels = in_weight.shape[1] * cols
    fits = tokens.shape[1] % (8 * peers) == 0 and in_weight.shape[0] % 128 == 0 and out_weight.shape[1] % 128 == 0
    if peers == 16 and cols == 2 and channels == 32 * peers and fits:
        return body_cube(tokens, norm_gain, in_weight, out_weight)
    return body_general(tokens, norm_gain, in_weight, out_weight)


def solution(mesh):
    in_specs = (P("col", "row", None), P(), P("row", "col"), P("col", "row"))
    out_specs = P("col", "row", None)
    return jax.shard_map(body, mesh=mesh, in_specs=in_specs, out_specs=out_specs, check_vma=False)
```

```python
import math

import jax
import jax.numpy as jnp
import numpy as np
from jax import lax
from jax.experimental import pallas as pl
from jax.experimental.pallas import tpu as pltpu
from jax.sharding import PartitionSpec as P


GS = 64
EPS = 1e-06
BF = jnp.bfloat16
F32 = jnp.float32


def angles(left, right, modulus):
    product = np.outer(np.asarray(left, np.int64), np.asarray(right, np.int64)) % modulus
    radians = product.astype(np.float64) * (2.0 * math.pi / modulus)
    return np.cos(radians), np.sin(radians)


def group_tables():
    cos, sin = angles(np.arange(GS), np.arange(GS), GS)
    half = GS // 2
    split = np.concatenate([cos[:, : half + 1], sin[:, 1:half]], axis=1)
    join = np.zeros((GS, GS))
    for j in range(half + 1):
        join[j, j] = 1.0
    for j in range(1, half):
        join[half + j, j] = -1.0
        join[j, GS - j] = 1.0
        join[half + j, GS - j] = 1.0
    return split, join


def spread_half(shard, peers):
    near = peers // 2
    other = lax.ppermute(shard, "row", [(i, i ^ near) for i in range(peers)])
    upper = lax.axis_index("row") >= near
    both = jnp.stack([jnp.where(upper, other, shard), jnp.where(upper, shard, other)])
    copies = jnp.broadcast_to(both[None], (near,) + both.shape)
    groups = [list(range(near)), list(range(near, peers))]
    got = lax.all_to_all(copies, "row", split_axis=0, concat_axis=0, tiled=True, axis_index_groups=groups)
    return got.transpose(1, 0, *range(2, got.ndim)).reshape((peers,) + shard.shape)


def column_parts(own, cols):
    if cols == 2:
        return [own, lax.ppermute(own, "col", [(0, 1), (1, 0)])]
    got = lax.all_gather(own, "col", axis=0, tiled=False)
    return [got[i] for i in range(cols)]


def dot(a, b, dims=((1,), (0,))):
    return lax.dot_general(a, b, (dims, ((), ())), preferred_element_type=F32)


def body_general(tokens, norm_gain, in_weight, out_weight):
    peers = lax.axis_size("row")
    cols = lax.axis_size("col")
    rows = tokens.shape[1]
    length = rows * peers
    channels = in_weight.shape[1] * cols
    narrow = channels // peers
    inner = rows // peers

    in_own = spread_half(in_weight, peers)
    in_own = in_own.reshape(-1, in_weight.shape[1])
    in_parts = column_parts(in_own, cols)
    out_own = spread_half(out_weight, peers)
    out_own = out_own.transpose(1, 0, 2).reshape(out_weight.shape[0], -1)
    out_parts = column_parts(out_own, cols)

    own_rows = tokens[0].astype(F32)
    inverse_rms = lax.rsqrt(jnp.mean(own_rows * own_rows, axis=-1, keepdims=True) + EPS)
    normed = (own_rows * inverse_rms * norm_gain.astype(F32)).astype(BF)
    projected = jnp.concatenate([dot(normed, part).astype(BF) for part in in_parts], axis=1)

    split, join = group_tables()
    groups = channels // GS
    split_all = jnp.asarray(np.kron(np.eye(groups), split.T), BF)
    join_all = jnp.asarray(np.kron(np.eye(groups), join), BF)
    sums = dot(split_all, projected, ((1,), (1,))).astype(BF)

    got = lax.all_to_all(sums.reshape(peers, narrow, rows), "row", split_axis=0, concat_axis=0, tiled=True)
    small_cos, small_sin = angles(np.arange(peers), np.arange(peers), peers)
    first = jnp.asarray(np.kron(np.concatenate([small_cos, -small_sin]), np.eye(narrow)), BF)
    stage = dot(first, got.reshape(channels, rows)).reshape(2, peers, narrow, rows)
    turn_cos, turn_sin = angles(np.arange(peers), np.arange(rows), length)
    turn_cos = jnp.asarray(turn_cos[:, None, :], F32)
    turn_sin = jnp.asarray(turn_sin[:, None, :], F32)
    real = stage[0] * turn_cos + stage[1] * turn_sin
    imag = stage[1] * turn_cos - stage[0] * turn_sin
    which = (lax.axis_index("row") * narrow + jnp.arange(narrow, dtype=jnp.int32)) % GS
    sine = (which > GS // 2)[None, :, None]
    lead = jnp.where(sine, -imag, real)
    tail = jnp.where(sine, real, imag)
    turned = jnp.concatenate([lead, tail], axis=-1).astype(BF).reshape(channels, 2 * rows)
    long_cos, long_sin = angles(np.arange(rows), np.arange(rows), rows)
    second = jnp.asarray(np.concatenate([long_cos, long_sin], axis=1), BF)
    whole = dot(second, turned, ((1,), (1,))).astype(BF)

    back = lax.all_to_all(whole.reshape(peers, inner, channels), "row", split_axis=0, concat_axis=0, tiled=True)
    back = back.reshape(peers, inner, peers, narrow).transpose(1, 2, 0, 3).reshape(rows, channels)
    mixed_real = (dot(back, join_all) * (1.0 / math.sqrt(length * GS))).astype(BF)
    width = channels // len(out_parts)
    result = sum(
        dot(mixed_real[:, i * width : (i + 1) * width], part) for i, part in enumerate(out_parts)
    )
    return result.astype(BF)[None]


def swap(value, axis, count, bit):
    return lax.ppermute(value, axis, [(i, i ^ bit) for i in range(count)])


def vmem_params():
    return pltpu.CompilerParams(vmem_limit_bytes=24 * 2**20)


def whole_specs(count):
    return [pl.BlockSpec(memory_space=pltpu.VMEM)] * count


def cost(flops, moved):
    return pl.CostEstimate(flops=int(flops), bytes_accessed=int(moved), transcendentals=0)


def norm_kernel(tokens_ref, gain_ref, out_ref):
    rows = tokens_ref[0].astype(F32)
    inverse_rms = lax.rsqrt(jnp.mean(rows * rows, axis=-1, keepdims=True) + EPS)
    out_ref[...] = (rows * inverse_rms * gain_ref[...].astype(F32)).astype(BF)


def norm_rows(tokens, gain):
    rows, width = tokens.shape[1:]
    step = rows // 6
    return pl.pallas_call(
        norm_kernel,
        out_shape=jax.ShapeDtypeStruct((rows, width), BF),
        grid=(rows // step,),
        in_specs=[
            pl.BlockSpec((1, step, width), lambda i: (0, i, 0)),
            pl.BlockSpec((1, width), lambda i: (0, 0)),
        ],
        out_specs=pl.BlockSpec((step, width), lambda i: (i, 0)),
        compiler_params=vmem_params(),
        cost_estimate=cost(rows * width * 2000, rows * width * 4),
        name="norm_rows",
    )(tokens, gain.reshape(1, width))


def spread_kernel(near, shard_ref, out_ref):
    for i in range(near):
        out_ref[i] = shard_ref[...]


def spread(shard, near):
    return pl.pallas_call(
        lambda *refs: spread_kernel(near, *refs),
        out_shape=jax.ShapeDtypeStruct((near,) + shard.shape, shard.dtype),
        in_specs=whole_specs(1),
        out_specs=pl.BlockSpec(memory_space=pltpu.VMEM),
        compiler_params=vmem_params(),
        cost_estimate=cost(shard.size * 400, shard.size * 2 * near),
        name="spread",
    )(shard)


def project_near(me, normed, own, other):
    near, depth, columns = own.shape
    rows = normed.shape[0]
    span = near * depth

    def kernel(me_ref, normed_ref, own_ref, other_ref, out_ref):
        piece = normed_ref[:, pl.ds(pl.multiple_of(me_ref[0] // near * span, span), span)]
        for i, ref in enumerate((own_ref, other_ref)):
            weight = ref[...].reshape(span, columns)
            out_ref[:, i * columns : (i + 1) * columns] = jnp.dot(piece, weight, preferred_element_type=F32)

    return pl.pallas_call(
        kernel,
        out_shape=jax.ShapeDtypeStruct((rows, 2 * columns), F32),
        in_specs=[pl.BlockSpec(memory_space=pltpu.SMEM)] + whole_specs(3),
        out_specs=pl.BlockSpec(memory_space=pltpu.VMEM),
        compiler_params=vmem_params(),
        cost_estimate=cost(4 * rows * span * columns, rows * span * 2),
        name="project_near",
    )(me, normed, own, other)


def project_far(me, normed, weight, split, sofar, half, into=None):
    near, depth, columns = weight.shape
    rows = normed.shape[0]
    span = near * depth

    def kernel(me_ref, normed_ref, weight_ref, split_ref, sofar_ref, *rest):
        piece = normed_ref[:, pl.ds(pl.multiple_of((1 - me_ref[0] // near) * span, span), span)]
        total = jnp.dot(piece, weight_ref[...].reshape(span, columns), preferred_element_type=F32)
        total = (total + sofar_ref[...]).astype(BF)
        rest[-1][...] = dot(split_ref[...], total, ((1,), (1,))).astype(BF)

    args = [me, normed, weight, split, sofar] + ([] if into is None else [into])
    extra = [] if into is None else [pl.BlockSpec(memory_space=pl.ANY)]
    zero = lambda i: (0, 0)
    return pl.pallas_call(
        kernel,
        out_shape=jax.ShapeDtypeStruct((2 * columns, rows), BF),
        grid=(1,),
        in_specs=[
            pl.BlockSpec(memory_space=pltpu.SMEM),
            pl.BlockSpec(normed.shape, zero),
            pl.BlockSpec(weight.shape, lambda i: (0, 0, 0)),
            pl.BlockSpec(split.shape, zero),
            pl.BlockSpec((rows, columns), lambda i: (0, half)),
        ]
        + extra,
        out_specs=pl.BlockSpec((columns, rows), lambda i: (half, 0)),
        input_output_aliases={} if into is None else {5: 0},
        compiler_params=vmem_params(),
        cost_estimate=cost(2 * rows * span * columns, weight.size * 2),
        name="project_far",
    )(*args)


def transform_kernel(narrow, me_ref, got_ref, first_ref, cos_ref, sin_ref, second_ref, out_ref):
    peers, _, rows = cos_ref.shape
    stage = jnp.dot(first_ref[...], got_ref[...], preferred_element_type=F32)
    stage = stage.reshape(2, peers, narrow, rows)
    cos, sin = cos_ref[...], sin_ref[...]
    real = stage[0] * cos + stage[1] * sin
    imag = stage[1] * cos - stage[0] * sin
    which = lax.broadcasted_iota(jnp.int32, (1, narrow, rows), 1) + me_ref[0] * narrow
    sine = lax.rem(which, GS) > GS // 2
    lead = jnp.where(sine, -imag, real).reshape(peers * narrow, rows).astype(BF)
    tail = jnp.where(sine, real, imag).reshape(peers * narrow, rows).astype(BF)
    lanes = ((1,), (1,))
    out = dot(second_ref[:, :rows], lead, lanes) + dot(second_ref[:, rows:], tail, lanes)
    out_ref[...] = out.astype(BF)


def transform(me, got, peers, rows):
    channels = got.shape[0]
    narrow = channels // peers
    small_cos, small_sin = angles(np.arange(peers), np.arange(peers), peers)
    first = jnp.asarray(np.kron(np.concatenate([small_cos, -small_sin]), np.eye(narrow)), BF)
    turn_cos, turn_sin = angles(np.arange(peers), np.arange(rows), rows * peers)
    long_cos, long_sin = angles(np.arange(rows), np.arange(rows), rows)
    second = jnp.asarray(np.concatenate([long_cos, long_sin], axis=1), BF)
    turns = [jnp.asarray(t[:, None, :], F32) for t in (turn_cos, turn_sin)]

    def kernel(*refs):
        transform_kernel(narrow, *refs)

    return pl.pallas_call(
        kernel,
        out_shape=jax.ShapeDtypeStruct((rows, channels), BF),
        in_specs=[pl.BlockSpec(memory_space=pltpu.SMEM)] + whole_specs(5),
        out_specs=pl.BlockSpec(memory_space=pltpu.VMEM),
        compiler_params=vmem_params(),
        cost_estimate=cost(4 * rows * channels * channels, 6 * channels * channels),
        name="transform",
    )(me, got, first, *turns, second)


def regroup(quads, lane):
    low, high = [], []
    for j in range(2):
        a, b = quads[j], quads[j + 2]
        low.append(jnp.where(lane < 64, a, pltpu.roll(b, 64, 1)))
        high.append(jnp.where(lane < 64, pltpu.roll(a, 64, 1), b))
    out = []
    even = lax.rem(lane, 64) < 32
    for e, o in (low, high):
        out.append(jnp.where(even, e, pltpu.roll(o, 32, 1)))
        out.append(jnp.where(even, pltpu.roll(e, 96, 1), o))
    return out


def output_kernel(scale, depth, me_ref, back_ref, join_ref, *refs):
    own, other, (out_ref, sheet) = refs[:8], refs[8:16], refs[16:]
    peers, inner, channels = back_ref.shape
    lane = lax.broadcasted_iota(jnp.int32, (inner, 128), 1)
    quads = channels // 128
    for a in range(quads):
        made = []
        for b in range(quads):
            tiles = [back_ref[4 * b + j, :, 128 * a : 128 * a + 128].astype(F32) for j in range(4)]
            made.append(regroup(tiles, lane))
        for i in range(4):
            for b in range(quads):
                sheet[b, pl.ds(4 * a + i, inner, stride=peers), :] = made[b][i]
    lines = jnp.concatenate([sheet[b].astype(BF) for b in range(quads)], axis=1)
    mixed_real = jnp.dot(lines, join_ref[...], preferred_element_type=F32) * scale
    mixed_real = mixed_real.astype(BF)
    near = len(own)
    upper = me_ref[0] // near
    place = lax.rem(me_ref[0], near)
    width = own[0].shape[2]
    for m in range(near):
        left = jnp.concatenate([own[m][0], own[m][1]], axis=1)
        right = jnp.concatenate([other[m][0], other[m][1]], axis=1)
        part = jnp.dot(mixed_real[:, :depth], left, preferred_element_type=F32)
        part = part + jnp.dot(mixed_real[:, depth:], right, preferred_element_type=F32)
        part = part.astype(BF)
        at = lax.bitwise_xor(place, m)
        here = pl.multiple_of((upper * near + at) * width, width)
        there = pl.multiple_of(((1 - upper) * near + at) * width, width)
        out_ref[:, pl.ds(here, width)] = part[:, :width]
        out_ref[:, pl.ds(there, width)] = part[:, width:]


def output(me, back, join, own, other, scale):
    peers, inner, channels = back.shape
    depth, width = own[0].shape[1:]
    rows = peers * inner

    def kernel(*refs):
        output_kernel(scale, depth, *refs)

    return pl.pallas_call(
        kernel,
        out_shape=jax.ShapeDtypeStruct((rows, width * peers), BF),
        in_specs=[pl.BlockSpec(memory_space=pltpu.SMEM)] + whole_specs(2 + len(own) + len(other)),
        out_specs=pl.BlockSpec(memory_space=pltpu.VMEM),
        scratch_shapes=[pltpu.VMEM((channels // 128, rows, 128), F32)],
        compiler_params=vmem_params(),
        cost_estimate=cost(2 * rows * channels * width * peers, rows * width * peers * 2),
        name="output",
    )(me, back, join, *own, *other)


def body_cube(tokens, norm_gain, in_weight, out_weight):
    peers = lax.axis_size("row")
    cols = lax.axis_size("col")
    near = peers // 2
    rows = tokens.shape[1]
    channels = in_weight.shape[1] * cols
    narrow = channels // peers
    inner = rows // peers
    me = lax.axis_index("row").astype(jnp.int32).reshape(1)
    split, join = group_tables()
    split_half = jnp.asarray(np.kron(np.eye(channels // cols // GS), split.T), BF)
    join_all = jnp.asarray(np.kron(np.eye(channels // GS), join), BF)

    def row_swap(value, bit):
        return swap(value, "row", peers, bit)

    def core_swap(value):
        return swap(value, "col", cols, 1)

    groups = [list(range(near)), list(range(near, peers))]

    def near_all(copies):
        return lax.all_to_all(copies, "row", split_axis=0, concat_axis=0, tiled=True, axis_index_groups=groups)

    in_far = row_swap(in_weight, near)
    copies_a = spread(in_weight, near)
    in_a = near_all(copies_a)
    copies_b = spread(in_far, near)
    in_b = near_all(copies_b)
    normed = norm_rows(tokens, norm_gain)
    sofar = project_near(me, normed, in_a, core_swap(in_a))
    other_b = core_swap(in_b)

    out_far = row_swap(out_weight, near)
    pairs = {0: jnp.stack([out_weight, out_far])}
    for bit in (1, 2, 4):
        pairs[bit] = row_swap(pairs[0], bit)
    pairs[3] = row_swap(pairs[2], 1)
    pairs[6] = row_swap(pairs[4], 2)
    pairs[5] = row_swap(pairs[1], 4)
    pairs[7] = row_swap(pairs[6], 1)
    others = [core_swap(pairs[m]) for m in range(near)]

    sums = project_far(me, normed, in_b, split_half, sofar, 0)
    sums = project_far(me, normed, other_b, split_half, sofar, 1, sums)
    got = lax.all_to_all(sums.reshape(peers, narrow, rows), "row", split_axis=0, concat_axis=0, tiled=True)
    whole = transform(me, got.reshape(channels, rows), peers, rows)
    back = lax.all_to_all(whole.reshape(peers, inner, channels), "row", split_axis=0, concat_axis=0, tiled=True)
    scale = 1.0 / math.sqrt(rows * peers * GS)
    result = output(me, back, join_all, [pairs[m] for m in range(near)], others, scale)
    return result[None]


def body(tokens, norm_gain, in_weight, out_weight):
    peers, cols = lax.axis_size("row"), lax.axis_size("col")
    channels = in_weight.shape[1] * cols
    fits = tokens.shape[1] % (8 * peers) == 0 and in_weight.shape[0] % 128 == 0 and out_weight.shape[1] % 128 == 0
    if peers == 16 and cols == 2 and channels == 32 * peers and fits:
        return body_cube(tokens, norm_gain, in_weight, out_weight)
    return body_general(tokens, norm_gain, in_weight, out_weight)


def solution(mesh):
    in_specs = (P("col", "row", None), P(), P("row", "col"), P("col", "row"))
    out_specs = P("col", "row", None)
    return jax.shard_map(body, mesh=mesh, in_specs=in_specs, out_specs=out_specs, check_vma=False)
```

```python
import math

import jax
import jax.numpy as jnp
import numpy as np
from jax import lax
from jax.experimental import pallas as pl
from jax.experimental.pallas import tpu as pltpu
from jax.sharding import PartitionSpec as P


GS = 64
EPS = 1e-06
BF = jnp.bfloat16
F32 = jnp.float32


def angles(left, right, modulus):
    product = np.outer(np.asarray(left, np.int64), np.asarray(right, np.int64)) % modulus
    radians = product.astype(np.float64) * (2.0 * math.pi / modulus)
    return np.cos(radians), np.sin(radians)


def group_tables():
    cos, sin = angles(np.arange(GS), np.arange(GS), GS)
    half = GS // 2
    split = np.concatenate([cos[:, : half + 1], sin[:, 1:half]], axis=1)
    join = np.zeros((GS, GS))
    for j in range(half + 1):
        join[j, j] = 1.0
    for j in range(1, half):
        join[half + j, j] = -1.0
        join[j, GS - j] = 1.0
        join[half + j, GS - j] = 1.0
    return split, join


def spread_half(shard, peers):
    near = peers // 2
    other = lax.ppermute(shard, "row", [(i, i ^ near) for i in range(peers)])
    upper = lax.axis_index("row") >= near
    both = jnp.stack([jnp.where(upper, other, shard), jnp.where(upper, shard, other)])
    copies = jnp.broadcast_to(both[None], (near,) + both.shape)
    groups = [list(range(near)), list(range(near, peers))]
    got = lax.all_to_all(copies, "row", split_axis=0, concat_axis=0, tiled=True, axis_index_groups=groups)
    return got.transpose(1, 0, *range(2, got.ndim)).reshape((peers,) + shard.shape)


def column_parts(own, cols):
    if cols == 2:
        return [own, lax.ppermute(own, "col", [(0, 1), (1, 0)])]
    got = lax.all_gather(own, "col", axis=0, tiled=False)
    return [got[i] for i in range(cols)]


def dot(a, b, dims=((1,), (0,))):
    return lax.dot_general(a, b, (dims, ((), ())), preferred_element_type=F32)


def body_general(tokens, norm_gain, in_weight, out_weight):
    peers = lax.axis_size("row")
    cols = lax.axis_size("col")
    rows = tokens.shape[1]
    length = rows * peers
    channels = in_weight.shape[1] * cols
    narrow = channels // peers
    inner = rows // peers

    in_own = spread_half(in_weight, peers)
    in_own = in_own.reshape(-1, in_weight.shape[1])
    in_parts = column_parts(in_own, cols)
    out_own = spread_half(out_weight, peers)
    out_own = out_own.transpose(1, 0, 2).reshape(out_weight.shape[0], -1)
    out_parts = column_parts(out_own, cols)

    own_rows = tokens[0].astype(F32)
    inverse_rms = lax.rsqrt(jnp.mean(own_rows * own_rows, axis=-1, keepdims=True) + EPS)
    normed = (own_rows * inverse_rms * norm_gain.astype(F32)).astype(BF)
    projected = jnp.concatenate([dot(normed, part).astype(BF) for part in in_parts], axis=1)

    split, join = group_tables()
    groups = channels // GS
    split_all = jnp.asarray(np.kron(np.eye(groups), split.T), BF)
    join_all = jnp.asarray(np.kron(np.eye(groups), join), BF)
    sums = dot(split_all, projected, ((1,), (1,))).astype(BF)

    got = lax.all_to_all(sums.reshape(peers, narrow, rows), "row", split_axis=0, concat_axis=0, tiled=True)
    small_cos, small_sin = angles(np.arange(peers), np.arange(peers), peers)
    first = jnp.asarray(np.kron(np.concatenate([small_cos, -small_sin]), np.eye(narrow)), BF)
    stage = dot(first, got.reshape(channels, rows)).reshape(2, peers, narrow, rows)
    turn_cos, turn_sin = angles(np.arange(peers), np.arange(rows), length)
    turn_cos = jnp.asarray(turn_cos[:, None, :], F32)
    turn_sin = jnp.asarray(turn_sin[:, None, :], F32)
    real = stage[0] * turn_cos + stage[1] * turn_sin
    imag = stage[1] * turn_cos - stage[0] * turn_sin
    which = (lax.axis_index("row") * narrow + jnp.arange(narrow, dtype=jnp.int32)) % GS
    sine = (which > GS // 2)[None, :, None]
    lead = jnp.where(sine, -imag, real)
    tail = jnp.where(sine, real, imag)
    turned = jnp.concatenate([lead, tail], axis=-1).astype(BF).reshape(channels, 2 * rows)
    long_cos, long_sin = angles(np.arange(rows), np.arange(rows), rows)
    second = jnp.asarray(np.concatenate([long_cos, long_sin], axis=1), BF)
    whole = dot(second, turned, ((1,), (1,))).astype(BF)

    back = lax.all_to_all(whole.reshape(peers, inner, channels), "row", split_axis=0, concat_axis=0, tiled=True)
    back = back.reshape(peers, inner, peers, narrow).transpose(1, 2, 0, 3).reshape(rows, channels)
    mixed_real = (dot(back, join_all) * (1.0 / math.sqrt(length * GS))).astype(BF)
    width = channels // len(out_parts)
    result = sum(
        dot(mixed_real[:, i * width : (i + 1) * width], part) for i, part in enumerate(out_parts)
    )
    return result.astype(BF)[None]


def swap(value, axis, count, bit):
    return lax.ppermute(value, axis, [(i, i ^ bit) for i in range(count)])


def vmem_params():
    return pltpu.CompilerParams(vmem_limit_bytes=24 * 2**20)


def whole_specs(count):
    return [pl.BlockSpec(memory_space=pltpu.VMEM)] * count


def cost(flops, moved):
    return pl.CostEstimate(flops=int(flops), bytes_accessed=int(moved), transcendentals=0)


def norm_kernel(tokens_ref, gain_ref, out_ref):
    rows = tokens_ref[0].astype(F32)
    inverse_rms = lax.rsqrt(jnp.mean(rows * rows, axis=-1, keepdims=True) + EPS)
    out_ref[...] = (rows * inverse_rms * gain_ref[...].astype(F32)).astype(BF)


def norm_rows(tokens, gain):
    rows, width = tokens.shape[1:]
    step = rows // 6
    return pl.pallas_call(
        norm_kernel,
        out_shape=jax.ShapeDtypeStruct((rows, width), BF),
        grid=(rows // step,),
        in_specs=[
            pl.BlockSpec((1, step, width), lambda i: (0, i, 0)),
            pl.BlockSpec((1, width), lambda i: (0, 0)),
        ],
        out_specs=pl.BlockSpec((step, width), lambda i: (i, 0)),
        compiler_params=vmem_params(),
        cost_estimate=cost(rows * width * 2000, rows * width * 4),
        name="norm_rows",
    )(tokens, gain.reshape(1, width))


def spread_kernel(near, shard_ref, out_ref):
    for i in range(near):
        out_ref[i] = shard_ref[...]


def spread(shard, near):
    return pl.pallas_call(
        lambda *refs: spread_kernel(near, *refs),
        out_shape=jax.ShapeDtypeStruct((near,) + shard.shape, shard.dtype),
        in_specs=whole_specs(1),
        out_specs=pl.BlockSpec(memory_space=pltpu.VMEM),
        compiler_params=vmem_params(),
        cost_estimate=cost(shard.size * 400, shard.size * 2 * near),
        name="spread",
    )(shard)


def project_near(me, normed, own, other):
    near, depth, columns = own.shape
    rows = normed.shape[0]
    span = near * depth

    def kernel(me_ref, normed_ref, own_ref, other_ref, out_ref):
        piece = normed_ref[:, pl.ds(pl.multiple_of(me_ref[0] // near * span, span), span)]
        for i, ref in enumerate((own_ref, other_ref)):
            weight = ref[...].reshape(span, columns)
            out_ref[:, i * columns : (i + 1) * columns] = jnp.dot(piece, weight, preferred_element_type=F32)

    return pl.pallas_call(
        kernel,
        out_shape=jax.ShapeDtypeStruct((rows, 2 * columns), F32),
        in_specs=[pl.BlockSpec(memory_space=pltpu.SMEM)] + whole_specs(3),
        out_specs=pl.BlockSpec(memory_space=pltpu.VMEM),
        compiler_params=vmem_params(),
        cost_estimate=cost(4 * rows * span * columns, rows * span * 2),
        name="project_near",
    )(me, normed, own, other)


def project_own(me, normed, weight, split, sofar):
    near, depth, columns = weight.shape
    rows = normed.shape[0]
    span = near * depth

    def kernel(me_ref, normed_ref, weight_ref, split_ref, sofar_ref, out_ref):
        piece = normed_ref[:, pl.ds(pl.multiple_of((1 - me_ref[0] // near) * span, span), span)]
        total = jnp.dot(piece, weight_ref[...].reshape(span, columns), preferred_element_type=F32)
        total = (total + sofar_ref[:, :columns]).astype(BF)
        out_ref[...] = dot(split_ref[...], total, ((1,), (1,))).astype(BF)

    return pl.pallas_call(
        kernel,
        out_shape=jax.ShapeDtypeStruct((columns, rows), BF),
        in_specs=[pl.BlockSpec(memory_space=pltpu.SMEM)] + whole_specs(4),
        out_specs=pl.BlockSpec(memory_space=pltpu.VMEM),
        compiler_params=vmem_params(),
        cost_estimate=cost(2 * rows * span * columns, weight.size * 2),
        name="project_own",
    )(me, normed, weight, split, sofar)


def project_other(me, normed, weight, split, sofar, first):
    near, depth, columns = weight.shape
    rows = normed.shape[0]
    span = near * depth

    def kernel(me_ref, normed_ref, weight_ref, split_ref, sofar_ref, first_ref, out_ref):
        out_ref[:columns] = first_ref[...]
        piece = normed_ref[:, pl.ds(pl.multiple_of((1 - me_ref[0] // near) * span, span), span)]
        total = jnp.dot(piece, weight_ref[...].reshape(span, columns), preferred_element_type=F32)
        total = (total + sofar_ref[:, columns:]).astype(BF)
        out_ref[columns:] = dot(split_ref[...], total, ((1,), (1,))).astype(BF)

    return pl.pallas_call(
        kernel,
        out_shape=jax.ShapeDtypeStruct((2 * columns, rows), BF),
        in_specs=[pl.BlockSpec(memory_space=pltpu.SMEM)] + whole_specs(5),
        out_specs=pl.BlockSpec(memory_space=pltpu.VMEM),
        compiler_params=vmem_params(),
        cost_estimate=cost(2 * rows * span * columns, weight.size * 2),
        name="project_other",
    )(me, normed, weight, split, sofar, first)


def sixteen(lines):
    wave = [2.0 * math.pi * i / 16 for i in range(16)]
    total = [lines[r] + lines[r + 8] for r in range(8)]
    left = [lines[r] - lines[r + 8] for r in range(8)]
    inner = [total[r] + total[r + 4] for r in range(4)]
    outer = [total[r] - total[r + 4] for r in range(4)]
    real, imag = {}, {}
    even, odd = inner[0] + inner[2], inner[1] + inner[3]
    real[0], real[8] = even + odd, even - odd
    imag[0] = imag[8] = jnp.zeros_like(even)
    real[4], imag[4] = inner[0] - inner[2], inner[3] - inner[1]
    root = math.sqrt(0.5)
    less, more = (outer[1] - outer[3]) * root, (outer[1] + outer[3]) * root
    real[2], real[6] = outer[0] + less, outer[0] - less
    imag[2], imag[6] = -more - outer[2], outer[2] - more
    cosine = [left[r] - left[8 - r] for r in range(1, 4)]
    sine = [left[r] + left[8 - r] for r in range(1, 4)]
    for k in (1, 3, 5, 7):
        real[k] = left[0] + sum(cosine[r - 1] * math.cos(wave[r * k % 16]) for r in range(1, 4))
        middle = left[4] * math.sin(wave[4 * k % 16])
        imag[k] = -middle - sum(sine[r - 1] * math.sin(wave[r * k % 16]) for r in range(1, 4))
    return real, imag


def transform_kernel(length, me_ref, got_ref, second_ref, out_ref, lead_ref, tail_ref):
    channels, rows = got_ref.shape
    peers = length // rows
    narrow = channels // peers
    k = lax.broadcasted_iota(jnp.int32, (peers, rows), 0)
    m = lax.broadcasted_iota(jnp.int32, (peers, rows), 1)
    radians = lax.rem(k * m, length).astype(F32) * (2.0 * math.pi / length)
    cos, sin = jnp.cos(radians), jnp.sin(radians)
    high, wide = 16, 128
    for c in range(0, narrow, high):
        which = lax.broadcasted_iota(jnp.int32, (high, wide), 0) + me_ref[0] * narrow + c
        sums = lax.rem(which, GS) > GS // 2
        for w in range(0, rows, wide):
            lines = [got_ref[r * narrow + c : r * narrow + c + high, w : w + wide].astype(F32) for r in range(peers)]
            real, imag = sixteen(lines)
            for f in range(peers):
                a, b = (real[f], imag[f]) if f <= peers // 2 else (real[peers - f], -imag[peers - f])
                tc, ts = cos[f : f + 1, w : w + wide], sin[f : f + 1, w : w + wide]
                first, other = a * tc + b * ts, b * tc - a * ts
                at = f * narrow + c
                lead_ref[at : at + high, w : w + wide] = jnp.where(sums, -other, first).astype(BF)
                tail_ref[at : at + high, w : w + wide] = jnp.where(sums, first, other).astype(BF)
    lanes = ((1,), (1,))
    out = dot(second_ref[:, :rows], lead_ref[...], lanes) + dot(second_ref[:, rows:], tail_ref[...], lanes)
    out_ref[...] = out.astype(BF)


def transform(me, got, peers, rows):
    channels = got.shape[0]
    long_cos, long_sin = angles(np.arange(rows), np.arange(rows), rows)
    second = jnp.asarray(np.concatenate([long_cos, long_sin], axis=1), BF)
    return pl.pallas_call(
        lambda *refs: transform_kernel(rows * peers, *refs),
        out_shape=jax.ShapeDtypeStruct((rows, channels), BF),
        in_specs=[pl.BlockSpec(memory_space=pltpu.SMEM)] + whole_specs(2),
        out_specs=pl.BlockSpec(memory_space=pltpu.VMEM),
        scratch_shapes=[pltpu.VMEM((channels, rows), BF), pltpu.VMEM((channels, rows), BF)],
        compiler_params=vmem_params(),
        cost_estimate=cost(4 * rows * channels * channels, 6 * channels * channels),
        name="transform",
    )(me, got, second)


def regroup(quads, lane):
    low, high = [], []
    for j in range(2):
        a, b = quads[j], quads[j + 2]
        low.append(jnp.where(lane < 64, a, pltpu.roll(b, 64, 1)))
        high.append(jnp.where(lane < 64, pltpu.roll(a, 64, 1), b))
    out = []
    even = lax.rem(lane, 64) < 32
    for e, o in (low, high):
        out.append(jnp.where(even, e, pltpu.roll(o, 32, 1)))
        out.append(jnp.where(even, pltpu.roll(e, 96, 1), o))
    return out


BLOCKS = {0: (0, 0), 4: (0, 2), 1: (1, 0), 5: (1, 2), 2: (2, 0), 6: (2, 2), 3: (3, 0), 7: (4, 0)}


def join_pattern(width):
    row = lax.broadcasted_iota(jnp.int32, (width, width), 0)
    column = lax.broadcasted_iota(jnp.int32, (width, width), 1)
    r, c = lax.rem(row, GS), lax.rem(column, GS)
    half = GS // 2
    cosine = r <= half
    order = jnp.where(cosine, r, r - half)
    straight = c == order
    turned = jnp.logical_and(c == GS - order, order < half)
    value = jnp.where(straight, jnp.where(cosine, 1.0, -1.0), jnp.where(turned, 1.0, 0.0))
    return jnp.where(row - r == column - c, value, 0.0).astype(BF)


def output_kernel(scale, depth, me_ref, back_ref, *refs):
    own, other, (out_ref, sheet, made_ref, out_sem) = refs[:5], refs[5:10], refs[10:]
    peers, inner, channels = back_ref.shape
    near = len(BLOCKS)
    width = own[0].shape[2]
    lane = lax.broadcasted_iota(jnp.int32, (inner, 128), 1)
    quads = channels // 128
    for a in range(quads):
        for b in range(quads):
            tiles = [back_ref[4 * b + j, :, 128 * a : 128 * a + 128].astype(F32) for j in range(4)]
            for i, tile in enumerate(regroup(tiles, lane)):
                sheet[b, pl.ds(4 * a + i, inner, stride=peers), :] = tile
    join = join_pattern(128)
    joined = [jnp.dot(sheet[b].astype(BF), join, preferred_element_type=F32) * scale for b in range(quads)]
    mixed_real = jnp.concatenate([part.astype(BF) for part in joined], axis=1)
    upper = me_ref[0] // near
    place = lax.rem(me_ref[0], near)
    stores = []
    for m, (source, start) in BLOCKS.items():
        left, right = [
            jnp.concatenate([arrays[source][start], arrays[source][start + 1]], axis=1) for arrays in (own, other)
        ]
        part = jnp.dot(mixed_real[:, :depth], left, preferred_element_type=F32)
        part = part + jnp.dot(mixed_real[:, depth:], right, preferred_element_type=F32)
        made_ref[m] = part.astype(BF)
        at = lax.bitwise_xor(place, m)
        for t, half in enumerate((upper, 1 - upper)):
            into = out_ref.at[:, pl.ds(pl.multiple_of((half * near + at) * width, width), width)]
            store = pltpu.make_async_copy(made_ref.at[m, :, t * width : t * width + width], into, out_sem.at[m, t])
            store.start()
            stores.append(store)
    for store in stores:
        store.wait()


def output(me, back, own, other, scale):
    peers, inner, channels = back.shape
    depth, width = own[0].shape[1:]
    rows = peers * inner
    near = len(BLOCKS)
    return pl.pallas_call(
        lambda *refs: output_kernel(scale, depth, *refs),
        out_shape=jax.ShapeDtypeStruct((rows, width * peers), BF),
        in_specs=[pl.BlockSpec(memory_space=pltpu.SMEM)] + whole_specs(1 + len(own) + len(other)),
        out_specs=pl.BlockSpec(memory_space=pltpu.HBM),
        scratch_shapes=[
            pltpu.VMEM((channels // 128, rows, 128), F32),
            pltpu.VMEM((near, rows, 2 * width), BF),
            pltpu.SemaphoreType.DMA((near, 2)),
        ],
        compiler_params=vmem_params(),
        cost_estimate=cost(2 * rows * channels * width * peers, rows * width * peers * 2),
        name="output",
    )(me, back, *own, *other)


def body_cube(tokens, norm_gain, in_weight, out_weight):
    peers = lax.axis_size("row")
    cols = lax.axis_size("col")
    near = peers // 2
    rows = tokens.shape[1]
    channels = in_weight.shape[1] * cols
    narrow = channels // peers
    inner = rows // peers
    me = lax.axis_index("row").astype(jnp.int32).reshape(1)
    split, _ = group_tables()
    split_half = jnp.asarray(np.kron(np.eye(channels // cols // GS), split.T), BF)

    def row_swap(value, bit):
        return swap(value, "row", peers, bit)

    def core_swap(value):
        return swap(value, "col", cols, 1)

    groups = [list(range(near)), list(range(near, peers))]

    def near_all(copies):
        return lax.all_to_all(copies, "row", split_axis=0, concat_axis=0, tiled=True, axis_index_groups=groups)

    in_far = row_swap(in_weight, near)
    copies_a = spread(in_weight, near)
    in_a = near_all(copies_a)
    copies_b = spread(in_far, near)
    in_b = near_all(copies_b)
    normed = norm_rows(tokens, norm_gain)
    sofar = project_near(me, normed, in_a, core_swap(in_a))
    other_b = core_swap(in_b)

    out_far = row_swap(out_weight, near)
    pair = jnp.stack([out_weight, out_far])
    beside = row_swap(pair, 4)
    quad = jnp.concatenate([pair, beside])
    over_x = row_swap(quad, 1)
    over_y = row_swap(quad, 2)
    over_xy = [row_swap(over_y[:2], 1), row_swap(over_x[2:], 2)]
    ours = [quad, over_x, over_y, *over_xy]
    others = [core_swap(value) for value in ours]

    sums = project_own(me, normed, in_b, split_half, sofar)
    sums = project_other(me, normed, other_b, split_half, sofar, sums)
    got = lax.all_to_all(sums.reshape(peers, narrow, rows), "row", split_axis=0, concat_axis=0, tiled=True)
    whole = transform(me, got.reshape(channels, rows), peers, rows)
    back = lax.all_to_all(whole.reshape(peers, inner, channels), "row", split_axis=0, concat_axis=0, tiled=True)
    scale = 1.0 / math.sqrt(rows * peers * GS)
    result = output(me, back, ours, others, scale)
    return result[None]


def body(tokens, norm_gain, in_weight, out_weight):
    peers, cols = lax.axis_size("row"), lax.axis_size("col")
    channels = in_weight.shape[1] * cols
    fits = tokens.shape[1] % (8 * peers) == 0 and in_weight.shape[0] % 128 == 0 and out_weight.shape[1] % 128 == 0
    if peers == 16 and cols == 2 and channels == 32 * peers and fits:
        return body_cube(tokens, norm_gain, in_weight, out_weight)
    return body_general(tokens, norm_gain, in_weight, out_weight)


def solution(mesh):
    in_specs = (P("col", "row", None), P(), P("row", "col"), P("col", "row"))
    out_specs = P("col", "row", None)
    return jax.shard_map(body, mesh=mesh, in_specs=in_specs, out_specs=out_specs, check_vma=False)
```

```python
import math

import jax
import jax.numpy as jnp
import numpy as np
from jax import lax
from jax.experimental import pallas as pl
from jax.experimental.pallas import tpu as pltpu
from jax.sharding import PartitionSpec as P


GS = 64
EPS = 1e-06
BF = jnp.bfloat16
F32 = jnp.float32


def angles(left, right, modulus):
    product = np.outer(np.asarray(left, np.int64), np.asarray(right, np.int64)) % modulus
    radians = product.astype(np.float64) * (2.0 * math.pi / modulus)
    return np.cos(radians), np.sin(radians)


def group_tables():
    cos, sin = angles(np.arange(GS), np.arange(GS), GS)
    half = GS // 2
    split = np.concatenate([cos[:, : half + 1], sin[:, 1:half]], axis=1)
    join = np.zeros((GS, GS))
    for j in range(half + 1):
        join[j, j] = 1.0
    for j in range(1, half):
        join[half + j, j] = -1.0
        join[j, GS - j] = 1.0
        join[half + j, GS - j] = 1.0
    return split, join


def spread_half(shard, peers):
    near = peers // 2
    other = lax.ppermute(shard, "row", [(i, i ^ near) for i in range(peers)])
    upper = lax.axis_index("row") >= near
    both = jnp.stack([jnp.where(upper, other, shard), jnp.where(upper, shard, other)])
    copies = jnp.broadcast_to(both[None], (near,) + both.shape)
    groups = [list(range(near)), list(range(near, peers))]
    got = lax.all_to_all(copies, "row", split_axis=0, concat_axis=0, tiled=True, axis_index_groups=groups)
    return got.transpose(1, 0, *range(2, got.ndim)).reshape((peers,) + shard.shape)


def column_parts(own, cols):
    if cols == 2:
        return [own, lax.ppermute(own, "col", [(0, 1), (1, 0)])]
    got = lax.all_gather(own, "col", axis=0, tiled=False)
    return [got[i] for i in range(cols)]


def dot(a, b, dims=((1,), (0,))):
    return lax.dot_general(a, b, (dims, ((), ())), preferred_element_type=F32)


def body_general(tokens, norm_gain, in_weight, out_weight):
    peers = lax.axis_size("row")
    cols = lax.axis_size("col")
    rows = tokens.shape[1]
    length = rows * peers
    channels = in_weight.shape[1] * cols
    narrow = channels // peers
    inner = rows // peers

    in_own = spread_half(in_weight, peers)
    in_own = in_own.reshape(-1, in_weight.shape[1])
    in_parts = column_parts(in_own, cols)
    out_own = spread_half(out_weight, peers)
    out_own = out_own.transpose(1, 0, 2).reshape(out_weight.shape[0], -1)
    out_parts = column_parts(out_own, cols)

    own_rows = tokens[0].astype(F32)
    inverse_rms = lax.rsqrt(jnp.mean(own_rows * own_rows, axis=-1, keepdims=True) + EPS)
    normed = (own_rows * inverse_rms * norm_gain.astype(F32)).astype(BF)
    projected = jnp.concatenate([dot(normed, part).astype(BF) for part in in_parts], axis=1)

    split, join = group_tables()
    groups = channels // GS
    split_all = jnp.asarray(np.kron(np.eye(groups), split.T), BF)
    join_all = jnp.asarray(np.kron(np.eye(groups), join), BF)
    sums = dot(split_all, projected, ((1,), (1,))).astype(BF)

    got = lax.all_to_all(sums.reshape(peers, narrow, rows), "row", split_axis=0, concat_axis=0, tiled=True)
    small_cos, small_sin = angles(np.arange(peers), np.arange(peers), peers)
    first = jnp.asarray(np.kron(np.concatenate([small_cos, -small_sin]), np.eye(narrow)), BF)
    stage = dot(first, got.reshape(channels, rows)).reshape(2, peers, narrow, rows)
    turn_cos, turn_sin = angles(np.arange(peers), np.arange(rows), length)
    turn_cos = jnp.asarray(turn_cos[:, None, :], F32)
    turn_sin = jnp.asarray(turn_sin[:, None, :], F32)
    real = stage[0] * turn_cos + stage[1] * turn_sin
    imag = stage[1] * turn_cos - stage[0] * turn_sin
    which = (lax.axis_index("row") * narrow + jnp.arange(narrow, dtype=jnp.int32)) % GS
    sine = (which > GS // 2)[None, :, None]
    lead = jnp.where(sine, -imag, real)
    tail = jnp.where(sine, real, imag)
    turned = jnp.concatenate([lead, tail], axis=-1).astype(BF).reshape(channels, 2 * rows)
    long_cos, long_sin = angles(np.arange(rows), np.arange(rows), rows)
    second = jnp.asarray(np.concatenate([long_cos, long_sin], axis=1), BF)
    whole = dot(second, turned, ((1,), (1,))).astype(BF)

    back = lax.all_to_all(whole.reshape(peers, inner, channels), "row", split_axis=0, concat_axis=0, tiled=True)
    back = back.reshape(peers, inner, peers, narrow).transpose(1, 2, 0, 3).reshape(rows, channels)
    mixed_real = (dot(back, join_all) * (1.0 / math.sqrt(length * GS))).astype(BF)
    width = channels // len(out_parts)
    result = sum(
        dot(mixed_real[:, i * width : (i + 1) * width], part) for i, part in enumerate(out_parts)
    )
    return result.astype(BF)[None]


def swap(value, axis, count, bit):
    return lax.ppermute(value, axis, [(i, i ^ bit) for i in range(count)])


def row_index():
    return lax.axis_index("row").astype(jnp.int32)


def vmem_params():
    return pltpu.CompilerParams(vmem_limit_bytes=24 * 2**20)


def whole_specs(count):
    return [pl.BlockSpec(memory_space=pltpu.VMEM)] * count


def cost(flops, moved):
    return pl.CostEstimate(flops=int(flops), bytes_accessed=int(moved), transcendentals=0)


def norm_kernel(tokens_ref, gain_ref, out_ref):
    rows = tokens_ref[0].astype(F32)
    inverse_rms = lax.rsqrt(jnp.mean(rows * rows, axis=-1, keepdims=True) + EPS)
    out_ref[...] = (rows * inverse_rms * gain_ref[...].astype(F32)).astype(BF)


def norm_rows(tokens, gain):
    rows, width = tokens.shape[1:]
    step = rows // 6
    return pl.pallas_call(
        norm_kernel,
        out_shape=jax.ShapeDtypeStruct((rows, width), BF),
        grid=(rows // step,),
        in_specs=[
            pl.BlockSpec((1, step, width), lambda i: (0, i, 0)),
            pl.BlockSpec((1, width), lambda i: (0, 0)),
        ],
        out_specs=pl.BlockSpec((step, width), lambda i: (i, 0)),
        compiler_params=vmem_params(),
        cost_estimate=cost(rows * width * 2000, rows * width * 4),
        name="norm_rows",
    )(tokens, gain.reshape(1, width))


def features(normed_ref, me, near, depth, bits):
    at = me // near * near + lax.bitwise_xor(lax.rem(me, near), bits)
    across = lax.rem(at + near, 2 * near)
    return [normed_ref[:, pl.ds(pl.multiple_of(i * depth, depth), depth)] for i in (at, across)]


def project_most(normed, own, other, near):
    bits = list(own)
    depth, columns = own[0].shape[1:]
    rows = normed.shape[0]

    def kernel(normed_ref, *refs):
        out_ref = refs[-1]
        piece = jnp.concatenate([f for m in bits for f in features(normed_ref, row_index(), near, depth, m)], axis=1)
        for half in range(2):
            weight = [r[...].reshape(2 * depth, columns) for r in refs[half * len(bits) : (half + 1) * len(bits)]]
            product = jnp.dot(piece, jnp.concatenate(weight), preferred_element_type=F32)
            out_ref[:, half * columns : (half + 1) * columns] = product

    arrays = [own[m] for m in bits] + [other[m] for m in bits]
    return pl.pallas_call(
        kernel,
        out_shape=jax.ShapeDtypeStruct((rows, 2 * columns), F32),
        in_specs=whole_specs(1 + len(arrays)),
        out_specs=pl.BlockSpec(memory_space=pltpu.VMEM),
        compiler_params=vmem_params(),
        cost_estimate=cost(8 * rows * len(bits) * depth * columns, rows * columns * 8),
        name="project_most",
    )(normed, *arrays)


def project_last(normed, own, other, split, sofar, near):
    bits = list(own)
    depth, columns = own[bits[0]].shape[1:]
    rows = normed.shape[0]

    def kernel(normed_ref, split_ref, sofar_ref, *refs):
        out_ref = refs[-1]
        piece = jnp.concatenate([f for m in bits for f in features(normed_ref, row_index(), near, depth, m)], axis=1)
        for half in range(2):
            weight = [r[...].reshape(2 * depth, columns) for r in refs[half * len(bits) : (half + 1) * len(bits)]]
            total = jnp.dot(piece, jnp.concatenate(weight), preferred_element_type=F32)
            total = (total + sofar_ref[:, half * columns : (half + 1) * columns]).astype(BF)
            sums = dot(split_ref[...], total, ((1,), (1,)))
            out_ref[half * columns : (half + 1) * columns] = sums.astype(BF)

    arrays = [own[m] for m in bits] + [other[m] for m in bits]
    return pl.pallas_call(
        kernel,
        out_shape=jax.ShapeDtypeStruct((2 * columns, rows), BF),
        in_specs=whole_specs(3 + len(arrays)),
        out_specs=pl.BlockSpec(memory_space=pltpu.VMEM),
        compiler_params=vmem_params(),
        cost_estimate=cost(8 * rows * len(bits) * depth * columns, rows * columns * 4),
        name="project_last",
    )(normed, split, sofar, *arrays)


def sixteen(lines):
    wave = [2.0 * math.pi * i / 16 for i in range(16)]
    total = [lines[r] + lines[r + 8] for r in range(8)]
    left = [lines[r] - lines[r + 8] for r in range(8)]
    inner = [total[r] + total[r + 4] for r in range(4)]
    outer = [total[r] - total[r + 4] for r in range(4)]
    real, imag = {}, {}
    even, odd = inner[0] + inner[2], inner[1] + inner[3]
    real[0], real[8] = even + odd, even - odd
    imag[0] = imag[8] = jnp.zeros_like(even)
    real[4], imag[4] = inner[0] - inner[2], inner[3] - inner[1]
    root = math.sqrt(0.5)
    less, more = (outer[1] - outer[3]) * root, (outer[1] + outer[3]) * root
    real[2], real[6] = outer[0] + less, outer[0] - less
    imag[2], imag[6] = -more - outer[2], outer[2] - more
    cosine = [left[r] - left[8 - r] for r in range(1, 4)]
    sine = [left[r] + left[8 - r] for r in range(1, 4)]
    for k in (1, 3, 5, 7):
        real[k] = left[0] + sum(cosine[r - 1] * math.cos(wave[r * k % 16]) for r in range(1, 4))
        middle = left[4] * math.sin(wave[4 * k % 16])
        imag[k] = -middle - sum(sine[r - 1] * math.sin(wave[r * k % 16]) for r in range(1, 4))
    return real, imag


def transform_kernel(length, got_ref, second_ref, out_ref, lead_ref, tail_ref):
    channels, rows = got_ref.shape
    peers = length // rows
    narrow = channels // peers
    k = lax.broadcasted_iota(jnp.int32, (peers, rows), 0)
    m = lax.broadcasted_iota(jnp.int32, (peers, rows), 1)
    radians = lax.rem(k * m, length).astype(F32) * (2.0 * math.pi / length)
    cos, sin = jnp.cos(radians), jnp.sin(radians)
    high, wide = 16, 128
    for c in range(0, narrow, high):
        which = lax.broadcasted_iota(jnp.int32, (high, wide), 0) + row_index() * narrow + c
        sums = lax.rem(which, GS) > GS // 2
        for w in range(0, rows, wide):
            lines = [got_ref[r * narrow + c : r * narrow + c + high, w : w + wide].astype(F32) for r in range(peers)]
            real, imag = sixteen(lines)
            for f in range(peers):
                a, b = (real[f], imag[f]) if f <= peers // 2 else (real[peers - f], -imag[peers - f])
                tc, ts = cos[f : f + 1, w : w + wide], sin[f : f + 1, w : w + wide]
                first, other = a * tc + b * ts, b * tc - a * ts
                at = f * narrow + c
                lead_ref[at : at + high, w : w + wide] = jnp.where(sums, -other, first).astype(BF)
                tail_ref[at : at + high, w : w + wide] = jnp.where(sums, first, other).astype(BF)
    lanes = ((1,), (1,))
    out = dot(second_ref[:, :rows], lead_ref[...], lanes) + dot(second_ref[:, rows:], tail_ref[...], lanes)
    out_ref[...] = out.astype(BF)


def transform(got, peers, rows):
    channels = got.shape[0]
    long_cos, long_sin = angles(np.arange(rows), np.arange(rows), rows)
    second = jnp.asarray(np.concatenate([long_cos, long_sin], axis=1), BF)
    return pl.pallas_call(
        lambda *refs: transform_kernel(rows * peers, *refs),
        out_shape=jax.ShapeDtypeStruct((rows, channels), BF),
        in_specs=whole_specs(2),
        out_specs=pl.BlockSpec(memory_space=pltpu.VMEM),
        scratch_shapes=[pltpu.VMEM((channels, rows), BF), pltpu.VMEM((channels, rows), BF)],
        compiler_params=vmem_params(),
        cost_estimate=cost(4 * rows * channels * channels, 6 * channels * channels),
        name="transform",
    )(got, second)


def regroup(quads, lane):
    low, high = [], []
    for j in range(2):
        a, b = quads[j], quads[j + 2]
        low.append(jnp.where(lane < 64, a, pltpu.roll(b, 64, 1)))
        high.append(jnp.where(lane < 64, pltpu.roll(a, 64, 1), b))
    out = []
    even = lax.rem(lane, 64) < 32
    for e, o in (low, high):
        out.append(jnp.where(even, e, pltpu.roll(o, 32, 1)))
        out.append(jnp.where(even, pltpu.roll(e, 96, 1), o))
    return out


BLOCKS = {0: (0, 0), 4: (0, 2), 1: (1, 0), 5: (1, 2), 2: (2, 0), 6: (2, 2), 3: (3, 0), 7: (4, 0)}


def join_pattern(width):
    row = lax.broadcasted_iota(jnp.int32, (width, width), 0)
    column = lax.broadcasted_iota(jnp.int32, (width, width), 1)
    r, c = lax.rem(row, GS), lax.rem(column, GS)
    half = GS // 2
    cosine = r <= half
    order = jnp.where(cosine, r, r - half)
    straight = c == order
    turned = jnp.logical_and(c == GS - order, order < half)
    value = jnp.where(straight, jnp.where(cosine, 1.0, -1.0), jnp.where(turned, 1.0, 0.0))
    return jnp.where(row - r == column - c, value, 0.0).astype(BF)


def output_kernel(scale, depth, back_ref, *refs):
    own, other, (out_ref, sheet, made_ref, out_sem) = refs[:5], refs[5:10], refs[10:]
    peers, inner, channels = back_ref.shape
    near = len(BLOCKS)
    width = own[0].shape[2]
    lane = lax.broadcasted_iota(jnp.int32, (inner, 128), 1)
    quads = channels // 128
    for a in range(quads):
        for b in range(quads):
            tiles = [back_ref[4 * b + j, :, 128 * a : 128 * a + 128].astype(F32) for j in range(4)]
            for i, tile in enumerate(regroup(tiles, lane)):
                sheet[b, pl.ds(4 * a + i, inner, stride=peers), :] = tile
    join = join_pattern(128)
    joined = [jnp.dot(sheet[b].astype(BF), join, preferred_element_type=F32) * scale for b in range(quads)]
    mixed_real = jnp.concatenate([part.astype(BF) for part in joined], axis=1)
    upper = row_index() // near
    place = lax.rem(row_index(), near)
    stores = []
    for m, (source, start) in BLOCKS.items():
        left, right = [
            jnp.concatenate([arrays[source][start], arrays[source][start + 1]], axis=1) for arrays in (own, other)
        ]
        part = jnp.dot(mixed_real[:, :depth], left, preferred_element_type=F32)
        part = part + jnp.dot(mixed_real[:, depth:], right, preferred_element_type=F32)
        made_ref[m] = part.astype(BF)
        at = lax.bitwise_xor(place, m)
        for t, half in enumerate((upper, 1 - upper)):
            into = out_ref.at[:, pl.ds(pl.multiple_of((half * near + at) * width, width), width)]
            store = pltpu.make_async_copy(made_ref.at[m, :, t * width : t * width + width], into, out_sem.at[m, t])
            store.start()
            stores.append(store)
    for store in stores:
        store.wait()


def output(back, own, other, scale):
    peers, inner, channels = back.shape
    depth, width = own[0].shape[1:]
    rows = peers * inner
    near = len(BLOCKS)
    return pl.pallas_call(
        lambda *refs: output_kernel(scale, depth, *refs),
        out_shape=jax.ShapeDtypeStruct((rows, width * peers), BF),
        in_specs=whole_specs(1 + len(own) + len(other)),
        out_specs=pl.BlockSpec(memory_space=pltpu.HBM),
        scratch_shapes=[
            pltpu.VMEM((channels // 128, rows, 128), F32),
            pltpu.VMEM((near, rows, 2 * width), BF),
            pltpu.SemaphoreType.DMA((near, 2)),
        ],
        compiler_params=vmem_params(),
        cost_estimate=cost(2 * rows * channels * width * peers, rows * width * peers * 2),
        name="output",
    )(back, *own, *other)


ROUNDS = ((1, 0, 1), (2, 0, 2), (4, 0, 4), (5, 1, 4), (3, 2, 1), (6, 4, 2), (7, 5, 2))


LATE = (6, 7)


def body_cube(tokens, norm_gain, in_weight, out_weight):
    peers = lax.axis_size("row")
    cols = lax.axis_size("col")
    near = peers // 2
    rows = tokens.shape[1]
    channels = in_weight.shape[1] * cols
    narrow = channels // peers
    inner = rows // peers
    split, _ = group_tables()
    split_half = jnp.asarray(np.kron(np.eye(channels // cols // GS), split.T), BF)

    def row_swap(value, bit):
        return swap(value, "row", peers, bit)

    def core_swap(value):
        return swap(value, "col", cols, 1)

    in_far = row_swap(in_weight, near)
    normed = norm_rows(tokens, norm_gain)
    parts = {0: jnp.stack([in_weight, in_far])}
    for bits, source, bit in ROUNDS:
        parts[bits] = row_swap(parts[source], bit)
    mirror = {bits: core_swap(part) for bits, part in parts.items()}
    most = [bits for bits in parts if bits not in LATE]
    sofar = project_most(normed, {m: parts[m] for m in most}, {m: mirror[m] for m in most}, near)

    out_far = row_swap(out_weight, near)
    pair = jnp.stack([out_weight, out_far])
    beside = row_swap(pair, 4)
    quad = jnp.concatenate([pair, beside])
    over_x = row_swap(quad, 1)
    over_y = row_swap(quad, 2)
    over_xy = [row_swap(over_y[:2], 1), row_swap(over_x[2:], 2)]
    ours = [quad, over_x, over_y, *over_xy]
    others = [core_swap(value) for value in ours]

    sums = project_last(normed, {m: parts[m] for m in LATE}, {m: mirror[m] for m in LATE}, split_half, sofar, near)
    got = lax.all_to_all(sums.reshape(peers, narrow, rows), "row", split_axis=0, concat_axis=0, tiled=True)
    whole = transform(got.reshape(channels, rows), peers, rows)
    back = lax.all_to_all(whole.reshape(peers, inner, channels), "row", split_axis=0, concat_axis=0, tiled=True)
    scale = 1.0 / math.sqrt(rows * peers * GS)
    result = output(back, ours, others, scale)
    return result[None]


def body(tokens, norm_gain, in_weight, out_weight):
    peers, cols = lax.axis_size("row"), lax.axis_size("col")
    channels = in_weight.shape[1] * cols
    fits = tokens.shape[1] % (8 * peers) == 0 and in_weight.shape[0] % 128 == 0 and out_weight.shape[1] % 128 == 0
    if peers == 16 and cols == 2 and channels == 32 * peers and fits:
        return body_cube(tokens, norm_gain, in_weight, out_weight)
    return body_general(tokens, norm_gain, in_weight, out_weight)


def solution(mesh):
    in_specs = (P("col", "row", None), P(), P("row", "col"), P("col", "row"))
    out_specs = P("col", "row", None)
    return jax.shard_map(body, mesh=mesh, in_specs=in_specs, out_specs=out_specs, check_vma=False)
```

```python
import math

import jax
import jax.numpy as jnp
import numpy as np
from jax import lax
from jax.experimental import pallas as pl
from jax.experimental.pallas import tpu as pltpu
from jax.sharding import PartitionSpec as P


GS = 64
EPS = 1e-06
BF = jnp.bfloat16
F32 = jnp.float32


def angles(left, right, modulus):
    product = np.outer(np.asarray(left, np.int64), np.asarray(right, np.int64)) % modulus
    radians = product.astype(np.float64) * (2.0 * math.pi / modulus)
    return np.cos(radians), np.sin(radians)


def group_tables():
    cos, sin = angles(np.arange(GS), np.arange(GS), GS)
    half = GS // 2
    split = np.concatenate([cos[:, : half + 1], sin[:, 1:half]], axis=1)
    join = np.zeros((GS, GS))
    for j in range(half + 1):
        join[j, j] = 1.0
    for j in range(1, half):
        join[half + j, j] = -1.0
        join[j, GS - j] = 1.0
        join[half + j, GS - j] = 1.0
    return split, join


def spread_half(shard, peers):
    near = peers // 2
    other = lax.ppermute(shard, "row", [(i, i ^ near) for i in range(peers)])
    upper = lax.axis_index("row") >= near
    both = jnp.stack([jnp.where(upper, other, shard), jnp.where(upper, shard, other)])
    copies = jnp.broadcast_to(both[None], (near,) + both.shape)
    groups = [list(range(near)), list(range(near, peers))]
    got = lax.all_to_all(copies, "row", split_axis=0, concat_axis=0, tiled=True, axis_index_groups=groups)
    return got.transpose(1, 0, *range(2, got.ndim)).reshape((peers,) + shard.shape)


def column_parts(own, cols):
    if cols == 2:
        return [own, lax.ppermute(own, "col", [(0, 1), (1, 0)])]
    got = lax.all_gather(own, "col", axis=0, tiled=False)
    return [got[i] for i in range(cols)]


def dot(a, b, dims=((1,), (0,))):
    return lax.dot_general(a, b, (dims, ((), ())), preferred_element_type=F32)


def body_general(tokens, norm_gain, in_weight, out_weight):
    peers = lax.axis_size("row")
    cols = lax.axis_size("col")
    rows = tokens.shape[1]
    length = rows * peers
    channels = in_weight.shape[1] * cols
    narrow = channels // peers
    inner = rows // peers

    in_own = spread_half(in_weight, peers)
    in_own = in_own.reshape(-1, in_weight.shape[1])
    in_parts = column_parts(in_own, cols)
    out_own = spread_half(out_weight, peers)
    out_own = out_own.transpose(1, 0, 2).reshape(out_weight.shape[0], -1)
    out_parts = column_parts(out_own, cols)

    own_rows = tokens[0].astype(F32)
    inverse_rms = lax.rsqrt(jnp.mean(own_rows * own_rows, axis=-1, keepdims=True) + EPS)
    normed = (own_rows * inverse_rms * norm_gain.astype(F32)).astype(BF)
    projected = jnp.concatenate([dot(normed, part).astype(BF) for part in in_parts], axis=1)

    split, join = group_tables()
    groups = channels // GS
    split_all = jnp.asarray(np.kron(np.eye(groups), split.T), BF)
    join_all = jnp.asarray(np.kron(np.eye(groups), join), BF)
    sums = dot(split_all, projected, ((1,), (1,))).astype(BF)

    got = lax.all_to_all(sums.reshape(peers, narrow, rows), "row", split_axis=0, concat_axis=0, tiled=True)
    small_cos, small_sin = angles(np.arange(peers), np.arange(peers), peers)
    first = jnp.asarray(np.kron(np.concatenate([small_cos, -small_sin]), np.eye(narrow)), BF)
    stage = dot(first, got.reshape(channels, rows)).reshape(2, peers, narrow, rows)
    turn_cos, turn_sin = angles(np.arange(peers), np.arange(rows), length)
    turn_cos = jnp.asarray(turn_cos[:, None, :], F32)
    turn_sin = jnp.asarray(turn_sin[:, None, :], F32)
    real = stage[0] * turn_cos + stage[1] * turn_sin
    imag = stage[1] * turn_cos - stage[0] * turn_sin
    which = (lax.axis_index("row") * narrow + jnp.arange(narrow, dtype=jnp.int32)) % GS
    sine = (which > GS // 2)[None, :, None]
    lead = jnp.where(sine, -imag, real)
    tail = jnp.where(sine, real, imag)
    turned = jnp.concatenate([lead, tail], axis=-1).astype(BF).reshape(channels, 2 * rows)
    long_cos, long_sin = angles(np.arange(rows), np.arange(rows), rows)
    second = jnp.asarray(np.concatenate([long_cos, long_sin], axis=1), BF)
    whole = dot(second, turned, ((1,), (1,))).astype(BF)

    back = lax.all_to_all(whole.reshape(peers, inner, channels), "row", split_axis=0, concat_axis=0, tiled=True)
    back = back.reshape(peers, inner, peers, narrow).transpose(1, 2, 0, 3).reshape(rows, channels)
    mixed_real = (dot(back, join_all) * (1.0 / math.sqrt(length * GS))).astype(BF)
    width = channels // len(out_parts)
    result = sum(
        dot(mixed_real[:, i * width : (i + 1) * width], part) for i, part in enumerate(out_parts)
    )
    return result.astype(BF)[None]


def swap(value, axis, count, bit):
    return lax.ppermute(value, axis, [(i, i ^ bit) for i in range(count)])


def row_index():
    return lax.axis_index("row").astype(jnp.int32)


def vmem_params():
    return pltpu.CompilerParams(vmem_limit_bytes=24 * 2**20)


def whole_specs(count):
    return [pl.BlockSpec(memory_space=pltpu.VMEM)] * count


def cost(flops, moved):
    return pl.CostEstimate(flops=int(flops), bytes_accessed=int(moved), transcendentals=0)


def norm_kernel(tokens_ref, gain_ref, out_ref):
    rows = tokens_ref[0].astype(F32)
    inverse_rms = lax.rsqrt(jnp.mean(rows * rows, axis=-1, keepdims=True) + EPS)
    out_ref[...] = (rows * inverse_rms * gain_ref[...].astype(F32)).astype(BF)


def norm_rows(tokens, gain):
    rows, width = tokens.shape[1:]
    step = rows // 6
    return pl.pallas_call(
        norm_kernel,
        out_shape=jax.ShapeDtypeStruct((rows, width), BF),
        grid=(rows // step,),
        in_specs=[
            pl.BlockSpec((1, step, width), lambda i: (0, i, 0)),
            pl.BlockSpec((1, width), lambda i: (0, 0)),
        ],
        out_specs=pl.BlockSpec((step, width), lambda i: (i, 0)),
        compiler_params=vmem_params(),
        cost_estimate=cost(rows * width * 2000, rows * width * 4),
        name="norm_rows",
    )(tokens, gain.reshape(1, width))


def features(normed_ref, me, near, depth, bits):
    at = me // near * near + lax.bitwise_xor(lax.rem(me, near), bits)
    across = lax.rem(at + near, 2 * near)
    return [normed_ref[:, pl.ds(pl.multiple_of(i * depth, depth), depth)] for i in (at, across)]


def project_most(normed, own, other, near):
    bits = list(own)
    depth, columns = own[0].shape[1:]
    rows = normed.shape[0]

    def kernel(normed_ref, *refs):
        out_ref = refs[-1]
        piece = jnp.concatenate([f for m in bits for f in features(normed_ref, row_index(), near, depth, m)], axis=1)
        for half in range(2):
            weight = [r[...].reshape(2 * depth, columns) for r in refs[half * len(bits) : (half + 1) * len(bits)]]
            product = jnp.dot(piece, jnp.concatenate(weight), preferred_element_type=F32)
            out_ref[:, half * columns : (half + 1) * columns] = product

    arrays = [own[m] for m in bits] + [other[m] for m in bits]
    return pl.pallas_call(
        kernel,
        out_shape=jax.ShapeDtypeStruct((rows, 2 * columns), F32),
        in_specs=whole_specs(1 + len(arrays)),
        out_specs=pl.BlockSpec(memory_space=pltpu.VMEM),
        compiler_params=vmem_params(),
        cost_estimate=cost(8 * rows * len(bits) * depth * columns, rows * columns * 8),
        name="project_most",
    )(normed, *arrays)


def project_last(normed, own, other, split, sofar, near):
    bits = list(own)
    depth, columns = own[bits[0]].shape[1:]
    rows = normed.shape[0]

    def kernel(normed_ref, split_ref, sofar_ref, *refs):
        out_ref = refs[-1]
        piece = jnp.concatenate([f for m in bits for f in features(normed_ref, row_index(), near, depth, m)], axis=1)
        for half in range(2):
            weight = [r[...].reshape(2 * depth, columns) for r in refs[half * len(bits) : (half + 1) * len(bits)]]
            total = jnp.dot(piece, jnp.concatenate(weight), preferred_element_type=F32)
            total = (total + sofar_ref[:, half * columns : (half + 1) * columns]).astype(BF)
            sums = dot(split_ref[...], total, ((1,), (1,)))
            out_ref[half * columns : (half + 1) * columns] = sums.astype(BF)

    arrays = [own[m] for m in bits] + [other[m] for m in bits]
    return pl.pallas_call(
        kernel,
        out_shape=jax.ShapeDtypeStruct((2 * columns, rows), BF),
        in_specs=whole_specs(3 + len(arrays)),
        out_specs=pl.BlockSpec(memory_space=pltpu.VMEM),
        compiler_params=vmem_params(),
        cost_estimate=cost(8 * rows * len(bits) * depth * columns, rows * columns * 4),
        name="project_last",
    )(normed, split, sofar, *arrays)


def sixteen(lines):
    wave = [2.0 * math.pi * i / 16 for i in range(16)]
    total = [lines[r] + lines[r + 8] for r in range(8)]
    left = [lines[r] - lines[r + 8] for r in range(8)]
    inner = [total[r] + total[r + 4] for r in range(4)]
    outer = [total[r] - total[r + 4] for r in range(4)]
    real, imag = {}, {}
    even, odd = inner[0] + inner[2], inner[1] + inner[3]
    real[0], real[8] = even + odd, even - odd
    imag[0] = imag[8] = jnp.zeros_like(even)
    real[4], imag[4] = inner[0] - inner[2], inner[3] - inner[1]
    root = math.sqrt(0.5)
    less, more = (outer[1] - outer[3]) * root, (outer[1] + outer[3]) * root
    real[2], real[6] = outer[0] + less, outer[0] - less
    imag[2], imag[6] = -more - outer[2], outer[2] - more
    cosine = [left[r] - left[8 - r] for r in range(1, 4)]
    sine = [left[r] + left[8 - r] for r in range(1, 4)]
    for k in (1, 3, 5, 7):
        real[k] = left[0] + sum(cosine[r - 1] * math.cos(wave[r * k % 16]) for r in range(1, 4))
        middle = left[4] * math.sin(wave[4 * k % 16])
        imag[k] = -middle - sum(sine[r - 1] * math.sin(wave[r * k % 16]) for r in range(1, 4))
    return real, imag


def transform_kernel(length, got_ref, second_ref, out_ref, lead_ref, tail_ref):
    channels, rows = got_ref.shape
    peers = length // rows
    narrow = channels // peers
    turns = second_ref[rows : rows + peers].astype(F32) + second_ref[rows + peers :].astype(F32)
    cos, sin = turns[:, :rows], turns[:, rows:]
    high, wide = 16, 128
    for c in range(0, narrow, high):
        which = lax.broadcasted_iota(jnp.int32, (high, wide), 0) + row_index() * narrow + c
        sums = lax.rem(which, GS) > GS // 2
        for w in range(0, rows, wide):
            lines = [got_ref[r * narrow + c : r * narrow + c + high, w : w + wide].astype(F32) for r in range(peers)]
            real, imag = sixteen(lines)
            for f in range(peers):
                a, b = (real[f], imag[f]) if f <= peers // 2 else (real[peers - f], -imag[peers - f])
                tc, ts = cos[f : f + 1, w : w + wide], sin[f : f + 1, w : w + wide]
                first, other = a * tc + b * ts, b * tc - a * ts
                at = f * narrow + c
                lead_ref[at : at + high, w : w + wide] = jnp.where(sums, -other, first).astype(BF)
                tail_ref[at : at + high, w : w + wide] = jnp.where(sums, first, other).astype(BF)
    lanes = ((1,), (1,))
    out = dot(second_ref[:rows, :rows], lead_ref[...], lanes) + dot(second_ref[:rows, rows:], tail_ref[...], lanes)
    out_ref[...] = out.astype(BF)


def transform(got, peers, rows):
    channels = got.shape[0]
    long_cos, long_sin = angles(np.arange(rows), np.arange(rows), rows)
    second = np.concatenate([long_cos, long_sin], axis=1)
    turns = np.concatenate(angles(np.arange(peers), np.arange(rows), rows * peers), axis=1)
    high = turns.astype(BF).astype(np.float64)
    second = jnp.asarray(np.concatenate([second, high, turns - high]), BF)
    return pl.pallas_call(
        lambda *refs: transform_kernel(rows * peers, *refs),
        out_shape=jax.ShapeDtypeStruct((rows, channels), BF),
        in_specs=whole_specs(2),
        out_specs=pl.BlockSpec(memory_space=pltpu.VMEM),
        scratch_shapes=[pltpu.VMEM((channels, rows), BF), pltpu.VMEM((channels, rows), BF)],
        compiler_params=vmem_params(),
        cost_estimate=cost(4 * rows * channels * channels, 6 * channels * channels),
        name="transform",
    )(got, second)


def regroup(quads, lane):
    low, high = [], []
    for j in range(2):
        a, b = quads[j], quads[j + 2]
        low.append(jnp.where(lane < 64, a, pltpu.roll(b, 64, 1)))
        high.append(jnp.where(lane < 64, pltpu.roll(a, 64, 1), b))
    out = []
    even = lax.rem(lane, 64) < 32
    for e, o in (low, high):
        out.append(jnp.where(even, e, pltpu.roll(o, 32, 1)))
        out.append(jnp.where(even, pltpu.roll(e, 96, 1), o))
    return out


BLOCKS = {0: (0, 0), 4: (0, 2), 1: (1, 0), 5: (1, 2), 2: (2, 0), 6: (2, 2), 3: (3, 0), 7: (4, 0)}


def join_pattern(width):
    row = lax.broadcasted_iota(jnp.int32, (width, width), 0)
    column = lax.broadcasted_iota(jnp.int32, (width, width), 1)
    r, c = lax.rem(row, GS), lax.rem(column, GS)
    half = GS // 2
    cosine = r <= half
    order = jnp.where(cosine, r, r - half)
    straight = c == order
    turned = jnp.logical_and(c == GS - order, order < half)
    value = jnp.where(straight, jnp.where(cosine, 1.0, -1.0), jnp.where(turned, 1.0, 0.0))
    return jnp.where(row - r == column - c, value, 0.0).astype(BF)


def output_kernel(scale, back_ref, *refs):
    own, other, (out_ref, sheet, made_ref, out_sem) = refs[:5], refs[5:10], refs[10:]
    peers, inner, channels = back_ref.shape
    near = len(BLOCKS)
    width = own[0].shape[2]
    lane = lax.broadcasted_iota(jnp.int32, (inner, 128), 1)
    quads = channels // 128
    for a in range(quads):
        for b in range(quads):
            tiles = [back_ref[4 * b + j, :, 128 * a : 128 * a + 128].astype(F32) for j in range(4)]
            for i, tile in enumerate(regroup(tiles, lane)):
                sheet[b, pl.ds(4 * a + i, inner, stride=peers), :] = tile
    join = join_pattern(128)
    joined = [jnp.dot(sheet[b].astype(BF), join, preferred_element_type=F32) * scale for b in range(quads)]
    mixed_real = jnp.concatenate([part.astype(BF) for part in joined], axis=1)
    upper = row_index() // near
    place = lax.rem(row_index(), near)
    stores = []
    for m, (source, start) in BLOCKS.items():
        weight = jnp.concatenate(
            [jnp.concatenate([a[source][start], a[source][start + 1]], axis=1) for a in (own, other)]
        )
        made_ref[m] = jnp.dot(mixed_real, weight, preferred_element_type=F32).astype(BF)
        at = lax.bitwise_xor(place, m)
        for t, half in enumerate((upper, 1 - upper)):
            into = out_ref.at[:, pl.ds(pl.multiple_of((half * near + at) * width, width), width)]
            store = pltpu.make_async_copy(made_ref.at[m, :, t * width : t * width + width], into, out_sem.at[m, t])
            store.start()
            stores.append(store)
    for store in stores:
        store.wait()


def output(back, own, other, scale):
    peers, inner, channels = back.shape
    _, width = own[0].shape[1:]
    rows = peers * inner
    near = len(BLOCKS)
    return pl.pallas_call(
        lambda *refs: output_kernel(scale, *refs),
        out_shape=jax.ShapeDtypeStruct((rows, width * peers), BF),
        in_specs=whole_specs(1 + len(own) + len(other)),
        out_specs=pl.BlockSpec(memory_space=pltpu.HBM),
        scratch_shapes=[
            pltpu.VMEM((channels // 128, rows, 128), F32),
            pltpu.VMEM((near, rows, 2 * width), BF),
            pltpu.SemaphoreType.DMA((near, 2)),
        ],
        compiler_params=vmem_params(),
        cost_estimate=cost(2 * rows * channels * width * peers, rows * width * peers * 2),
        name="output",
    )(back, *own, *other)


ROUNDS = ((1, 0, 1), (2, 0, 2), (4, 0, 4), (5, 1, 4), (3, 2, 1), (6, 4, 2), (7, 5, 2))


LATE = (7,)


def body_cube(tokens, norm_gain, in_weight, out_weight):
    peers = lax.axis_size("row")
    cols = lax.axis_size("col")
    near = peers // 2
    rows = tokens.shape[1]
    channels = in_weight.shape[1] * cols
    narrow = channels // peers
    inner = rows // peers
    split, _ = group_tables()
    split_half = jnp.asarray(np.kron(np.eye(channels // cols // GS), split.T), BF)

    def row_swap(value, bit):
        return swap(value, "row", peers, bit)

    def core_swap(value):
        return swap(value, "col", cols, 1)

    in_far = row_swap(in_weight, near)
    normed = norm_rows(tokens, norm_gain)
    parts = {0: jnp.stack([in_weight, in_far])}
    for bits, source, bit in ROUNDS:
        parts[bits] = row_swap(parts[source], bit)
    mirror = {bits: core_swap(part) for bits, part in parts.items()}
    most = [bits for bits in parts if bits not in LATE]
    sofar = project_most(normed, {m: parts[m] for m in most}, {m: mirror[m] for m in most}, near)

    out_far = row_swap(out_weight, near)
    pair = jnp.stack([out_weight, out_far])
    beside = row_swap(pair, 4)
    quad = jnp.concatenate([pair, beside])
    over_x = row_swap(quad, 1)
    over_y = row_swap(quad, 2)
    over_xy = [row_swap(over_y[:2], 1), row_swap(over_x[2:], 2)]
    ours = [quad, over_x, over_y, *over_xy]
    others = [core_swap(value) for value in ours]

    sums = project_last(normed, {m: parts[m] for m in LATE}, {m: mirror[m] for m in LATE}, split_half, sofar, near)
    got = lax.all_to_all(sums.reshape(peers, narrow, rows), "row", split_axis=0, concat_axis=0, tiled=True)
    whole = transform(got.reshape(channels, rows), peers, rows)
    back = lax.all_to_all(whole.reshape(peers, inner, channels), "row", split_axis=0, concat_axis=0, tiled=True)
    scale = 1.0 / math.sqrt(rows * peers * GS)
    result = output(back, ours, others, scale)
    return result[None]


def body(tokens, norm_gain, in_weight, out_weight):
    peers, cols = lax.axis_size("row"), lax.axis_size("col")
    channels = in_weight.shape[1] * cols
    fits = tokens.shape[1] % (8 * peers) == 0 and in_weight.shape[0] % 128 == 0 and out_weight.shape[1] % 128 == 0
    if peers == 16 and cols == 2 and channels == 32 * peers and fits:
        return body_cube(tokens, norm_gain, in_weight, out_weight)
    return body_general(tokens, norm_gain, in_weight, out_weight)


def solution(mesh):
    in_specs = (P("col", "row", None), P(), P("row", "col"), P("col", "row"))
    out_specs = P("col", "row", None)
    return jax.shard_map(body, mesh=mesh, in_specs=in_specs, out_specs=out_specs, check_vma=False)
```
